256 devices in a mesh: sp: 32 (over z, y), fs: 4 (over x), tp: 2 (over core).
Axes of the slice: x: 4, y: 4, z: 8, core: 2. Of those that a mesh axis runs over, the one named last changes fastest.
Arguments:
- tokens: bfloat16 [16384, 2048], P('sp', ('fs', 'tp')), may hold values from -6 to 6
- in_gain: float32 [2048], replicated, may hold values from 0.1 to 1.9
- conv_a_weight: bfloat16 [2048, 1024], P(None, ('fs', 'tp')), may hold values from -0.125 to 0.125
- conv_gate_weight: bfloat16 [2048, 1024], P(None, ('fs', 'tp')), may hold values from -0.125 to 0.125
- query_weight: bfloat16 [2048, 1024], P(None, ('fs', 'tp')), may hold values from -0.125 to 0.125
- key_weight: bfloat16 [2048, 1024], P(None, ('fs', 'tp')), may hold values from -0.125 to 0.125
- value_weight: bfloat16 [2048, 1024], P(None, ('fs', 'tp')), may hold values from -0.125 to 0.125
- conv_taps: bfloat16 [31, 1024], replicated, may hold values from -3 to 3
- conv_norm_gain: float32 [1024], replicated, may hold values from 0.1 to 1.9
- break_shift: bfloat16 [16, 16384], P(('fs', 'tp'), 'sp'), may hold values from -20 to 1
- conv_out_gain: float32 [1024], replicated, may hold values from 0.1 to 1.9
- attn_out_gain: float32 [1024], replicated, may hold values from 0.1 to 1.9
- out_weight: bfloat16 [2048, 2048], P(None, ('fs', 'tp')), may hold values from -0.125 to 0.125
Outputs:
- mixed: bfloat16 [16384, 2048], P('sp', ('fs', 'tp'))
The draws below stay inside these ranges and needn't reach their ends.
All inputs are finite; a program needn't handle non-finite values.
Results may differ from the reference program's by a relative error of at most 0.0078.
Values may be sent and summed in bfloat16 or wider, within the bound.
A program may use at most 128 MiB of HBM per device.

```python
import math
import jax
import jax.numpy as jnp
from jax import lax

D = 2048
HEAD_DIM = 64
KERNEL = 31
TOK_DEV = 512
SEQUENCE_TOKENS = 16384
CONV_CH = 1024
SB_WIDTH = 1024
HEADS = 16


def draw_conv_taps(key, part):
    columns = jnp.arange(D // 2, dtype=jnp.float32) / (D // 2)
    entries = jnp.clip(jax.random.normal(key, (KERNEL, D // 2), jnp.float32), -4.0, 4.0)
    rising = 1.0 + 2.0 * columns
    return (entries * rising[None, :] * KERNEL ** (-0.5)).astype(jnp.bfloat16)


def draw_break_shift(key, part):
    key_sequence = jax.random.split(key, 5)
    count_of_heads = D // 2 // HEAD_DIM
    block_count = SEQUENCE_TOKENS // TOK_DEV
    slow_share = 0.5
    slow_heads = jax.random.uniform(key_sequence[0], (count_of_heads,), jnp.float32) < slow_share
    far_level = -math.log(SEQUENCE_TOKENS) - 0.5
    depth_tier = jnp.where(slow_heads, far_level, -3.0)
    block_factor = jnp.log(jax.random.uniform(key_sequence[1], (count_of_heads, block_count), jnp.float32, 0.5, 2.0))
    block_summand = jnp.repeat(block_factor, TOK_DEV, axis=1)
    coarse_estimate = jnp.clip(jax.random.normal(key_sequence[2], (count_of_heads, SEQUENCE_TOKENS), jnp.float32), -2.0, 2.0) * 0.5
    surge_groups = jax.random.uniform(key_sequence[3], (count_of_heads, SEQUENCE_TOKENS), jnp.float32) < 4.0 / SEQUENCE_TOKENS
    surge_depth = jax.random.uniform(key_sequence[4], (count_of_heads, SEQUENCE_TOKENS), jnp.float32, -1.5, 0.0)
    displaced_rows = jnp.where(surge_groups, surge_depth, depth_tier[:, None] + block_summand + coarse_estimate)
    return displaced_rows.astype(jnp.bfloat16)


def block_levels(own_key, extent, cuts, smallest, high):
    loudness = 1.0
    for dim, shards_of in cuts:
        heights = jax.random.uniform(jax.random.fold_in(jax.random.fold_in(own_key, 6), dim), (shards_of,), jnp.float32, smallest / len(cuts), high / len(cuts))
        loudness = loudness * jnp.repeat(jnp.exp(heights), extent[dim] // shards_of).reshape((-1,) + (1,) * (len(extent) - 1 - dim))
    return loudness


def bell_draw(key, extent, width, reach, cuts=(), kind=jnp.bfloat16):
    result = width * jax.random.normal(key, extent, jnp.float32)
    if cuts:
        result = result * block_levels(key, extent, cuts, -0.22, 0.18)
    return jnp.clip(result, -reach, reach).astype(kind)


def setup_inputs(seed: int = 0) -> dict:
    keys = jax.random.split(jax.random.key(seed), 14)
    return {
        "tokens": bell_draw(keys[0], (SEQUENCE_TOKENS, D), 1.0, 6.0, ((0, 32), (1, 8))),
        "in_gain": jnp.clip(1.0 + 0.18 * jax.random.normal(keys[1], (D,), jnp.float32), 0.1, 1.9),
        "conv_a_weight": bell_draw(keys[2], (D, CONV_CH), D ** -0.5, 0.125, ((1, 8),)),
        "conv_gate_weight": bell_draw(keys[3], (D, CONV_CH), D ** -0.5, 0.125, ((1, 8),)),
        "query_weight": bell_draw(keys[4], (D, SB_WIDTH), D ** -0.5, 0.125, ((1, 8),)),
        "key_weight": bell_draw(keys[5], (D, SB_WIDTH), D ** -0.5, 0.125, ((1, 8),)),
        "value_weight": bell_draw(keys[6], (D, SB_WIDTH), D ** -0.5, 0.125, ((1, 8),)),
        "conv_taps": draw_conv_taps(jax.random.fold_in(keys[13], 71), 0),
        "conv_norm_gain": jnp.clip(1.0 + 0.18 * jax.random.normal(keys[8], (CONV_CH,), jnp.float32), 0.1, 1.9),
        "break_shift": draw_break_shift(jax.random.fold_in(keys[13], 71), 0),
        "conv_out_gain": jnp.clip(1.0 + 0.18 * jax.random.normal(keys[10], (CONV_CH,), jnp.float32), 0.1, 1.9),
        "attn_out_gain": jnp.clip(1.0 + 0.18 * jax.random.normal(keys[11], (SB_WIDTH,), jnp.float32), 0.1, 1.9),
        "out_weight": bell_draw(keys[12], (D, D), D ** -0.5, 0.125, ((1, 8),)),
    }


epsilon = 1e-06

def project_rows(scaled_input, weight, input_scale):
    product = jnp.dot(scaled_input, weight, preferred_element_type=jnp.float32)
    return (product * input_scale).astype(jnp.bfloat16)

def branch_output(mixed_part, gain, rows):
    mixed_wide = mixed_part.astype(jnp.float32)
    branch_scale = lax.rsqrt(lax.optimization_barrier(jnp.mean(mixed_wide * mixed_wide, axis=1, keepdims=True)) + epsilon)
    scaled = (mixed_wide * gain[None, :]).astype(jnp.bfloat16)
    return jnp.dot(scaled, rows, preferred_element_type=jnp.float32) * branch_scale

def reference(tokens, in_gain, conv_a_weight, conv_gate_weight, query_weight, key_weight, value_weight, conv_taps, conv_norm_gain, break_shift, conv_out_gain, attn_out_gain, out_weight):
    tokens_wide = tokens.astype(jnp.float32)
    input_scale = lax.rsqrt(lax.optimization_barrier(jnp.mean(tokens_wide * tokens_wide, axis=1, keepdims=True)) + epsilon)
    scaled_input = (tokens_wide * in_gain[None, :]).astype(jnp.bfloat16)
    conv_a = project_rows(scaled_input, conv_a_weight, input_scale)
    conv_gate = project_rows(scaled_input, conv_gate_weight, input_scale)
    query = project_rows(scaled_input, query_weight, input_scale)
    key = project_rows(scaled_input, key_weight, input_scale)
    value = project_rows(scaled_input, value_weight, input_scale)
    gated_input = conv_a.astype(jnp.float32) * jax.nn.sigmoid(conv_gate.astype(jnp.float32))
    padded = jnp.pad(gated_input, ((KERNEL - 1, 0), (0, 0)))
    tap_values = conv_taps.astype(jnp.float32)
    conv_out = jnp.zeros((SEQUENCE_TOKENS, CONV_CH), jnp.float32)
    for offset in range(KERNEL):
        conv_out = conv_out + tap_values[offset][None, :] * padded[offset:offset + SEQUENCE_TOKENS]
    row_mean = lax.optimization_barrier(jnp.mean(conv_out, axis=1, keepdims=True))
    centered = conv_out - row_mean
    row_spread = lax.optimization_barrier(jnp.mean(centered * centered, axis=1, keepdims=True))
    normed = centered * lax.rsqrt(row_spread + epsilon) * conv_norm_gain[None, :]
    conv_mixed = jax.nn.silu(normed).astype(jnp.bfloat16)
    query_heads = query.astype(jnp.float32).reshape(SEQUENCE_TOKENS, HEADS, HEAD_DIM)
    key_heads = key.astype(jnp.float32).reshape(SEQUENCE_TOKENS, HEADS, HEAD_DIM)
    value_heads = value.astype(jnp.float32).reshape(SEQUENCE_TOKENS, HEADS, HEAD_DIM)
    shifts = break_shift.astype(jnp.float32)
    score_scale = HEAD_DIM ** (-0.5)
    block_count = SEQUENCE_TOKENS // TOK_DEV

    def one_block(block_index):
        first_query = (block_index * TOK_DEV).astype(jnp.int32)
        queries = lax.dynamic_slice_in_dim(query_heads, first_query, TOK_DEV, 0)
        query_pos = first_query + jnp.arange(TOK_DEV, dtype=jnp.int32)

        def advance(counter, running):
            outputs, behind = running
            begin_row = ((block_index - counter) * TOK_DEV).astype(jnp.int32)
            key_rows = lax.dynamic_slice_in_dim(key_heads, begin_row, TOK_DEV, 0)
            value_rows = lax.dynamic_slice_in_dim(value_heads, begin_row, TOK_DEV, 0)
            shift_rows = lax.dynamic_slice_in_dim(shifts, begin_row, TOK_DEV, 1)
            scores = jnp.einsum('qhd,khd->hqk', queries, key_rows) * score_scale
            scores = scores + shift_rows[:, None, :]
            key_pos = begin_row + jnp.arange(TOK_DEV, dtype=jnp.int32)
            allowed = (key_pos[None, :] < query_pos[:, None])[None]
            log_fail = jnp.where(allowed, jax.nn.log_sigmoid(-scores), 0.0)
            later_sum = lax.cumsum(log_fail, axis=2, reverse=True) - log_fail + behind[:, :, None]
            weights = jnp.where(allowed, jnp.exp(jax.nn.log_sigmoid(scores) + later_sum), 0.0).astype(jnp.bfloat16)
            weights = lax.optimization_barrier(weights).astype(jnp.float32)
            outputs = outputs + jnp.einsum('hqk,khd->qhd', weights, value_rows)
            return (outputs, behind + lax.optimization_barrier(jnp.sum(log_fail, axis=2)))
        start_state = (jnp.zeros((TOK_DEV, HEADS, HEAD_DIM), jnp.float32), jnp.zeros((HEADS, TOK_DEV), jnp.float32))
        outputs, behind = lax.fori_loop(0, block_index + 1, advance, start_state)
        return outputs
    blocks_out = lax.map(one_block, jnp.arange(block_count, dtype=jnp.int32))
    attn_mixed = blocks_out.reshape(SEQUENCE_TOKENS, SB_WIDTH).astype(jnp.bfloat16)
    total = branch_output(conv_mixed, conv_out_gain, out_weight[:CONV_CH])
    total = total + branch_output(attn_mixed, attn_out_gain, out_weight[CONV_CH:])
    return total.astype(jnp.bfloat16)
```

```python
import jax
import jax.numpy as jnp
from jax import lax
from jax.experimental import pallas as pl
from jax.experimental.pallas import tpu as pltpu
from jax.sharding import PartitionSpec as P

MESH = pl.DeviceIdType.MESH
VMEM = pltpu.VMEM
HEAD = 64
PLANES, BLOCKS, RING, CORES = 8, 4, 4, 2
SHIFT_ROWS = 16
epsilon = 1e-06
f32, bf16 = jnp.float32, jnp.bfloat16


def position():
    return lax.axis_index("sp"), lax.axis_index("fs"), lax.axis_index("tp")


def greet(devices):
    barrier = pltpu.get_barrier_semaphore()
    for device in devices:
        pl.semaphore_signal(barrier, inc=1, device_id=device, device_id_type=MESH)
    pl.semaphore_wait(barrier, len(devices))


def remote(src, dst, send, recv, device):
    return pltpu.make_async_remote_copy(
        src_ref=src, dst_ref=dst, send_sem=send, recv_sem=recv, device_id=device, device_id_type=MESH
    )


def left_lanes(shape):
    return lax.broadcasted_iota(jnp.int32, shape, 1) < HEAD


def swap_halves(x):
    return pltpu.roll(x, HEAD, 1)


class RowGather:
    steps = 9

    def __init__(self, own, whole, send, recv):
        self.own, self.whole, self.send, self.recv = own, whole, send, recv
        sp, x, c = position()
        self.x, self.c = x, c
        self.right = (sp, lax.rem(x + 1, RING), c)
        self.left = (sp, lax.rem(x + RING - 1, RING), c)
        self.partner = (sp, x, 1 - c)
        self.half = own.shape[0] // 2

    def index(self, dx, other=False):
        return CORES * lax.rem(self.x + dx + RING, RING) + (1 - self.c if other else self.c)

    def slot(self, dx, other=False, part=None):
        ref = self.whole.at[self.index(dx, other)]
        return ref if part is None else ref.at[pl.ds(part * self.half, self.half)]

    def copy(self, k, src, dst, device):
        return remote(src, dst, self.send.at[k], self.recv.at[k], device)

    def out(self, k):
        if k == 0:
            return self.copy(0, self.own, self.slot(0), self.right)
        if k == 1:
            return self.copy(1, self.own, self.slot(0), self.left)
        if k == 2:
            return self.copy(2, self.own, self.slot(0), self.partner)
        if k == 3:
            return self.copy(3, self.slot(-1, part=0), self.slot(-1, part=0), self.right)
        if k == 4:
            return self.copy(4, self.slot(1, part=1), self.slot(1, part=1), self.left)
        if k == 5:
            return self.copy(5, self.slot(-1), self.slot(-1), self.partner)
        if k == 6:
            return self.copy(6, self.slot(1), self.slot(1), self.partner)
        if k == 7:
            return self.copy(7, self.slot(2, part=0), self.slot(2, part=0), self.partner)
        return self.copy(8, self.slot(2, part=1), self.slot(2, part=1), self.partner)

    def arrived(self, k):
        slots = (
            (-1, False, None),
            (1, False, None),
            (0, True, None),
            (2, False, 0),
            (2, False, 1),
            (-1, True, None),
            (1, True, None),
            (2, True, 0),
            (2, True, 1),
        )
        slot = self.slot(*slots[k])
        self.copy(k, slot, slot, self.partner).wait_recv()

    def start(self):
        for k in (0, 1, 2):
            self.out(k).start()

    def relay_near(self):
        self.arrived(0)
        self.out(3).start()
        self.out(5).start()
        self.arrived(1)
        self.out(4).start()
        self.out(6).start()

    def relay_far(self):
        self.arrived(3)
        self.out(7).start()
        self.arrived(4)
        self.out(8).start()

    def sent(self):
        for k in range(self.steps):
            self.out(k).wait_send()


def project_kernel(
    tok, gain, shift, taps, wa, wg, wq, wk, wv,
    conv_out, kvs, qs,
    whole, stacked, acc, squares, padded, tail, halo, weight_sem, send, recv, halo_send, halo_recv,
):
    sp, x, c = position()
    count = lax.axis_size("sp")
    rows, width = tok.shape
    local = wa.shape[1]
    loads = [
        pltpu.make_async_copy(w, stacked.at[:, pl.ds(local * i, local)], weight_sem.at[i])
        for i, w in enumerate((wa, wg, wq, wk, wv))
    ]
    for load in loads:
        load.start()
    later = (lax.rem(sp + 1, count), x, c)
    before = (lax.rem(sp + count - 1, count), x, c)
    net = RowGather(tok, whole, send, recv)
    greet([net.right, net.left, net.partner, later, before])
    net.start()
    for load in loads:
        load.wait()
    tile = 128

    def piece(ref, index, first=False):
        weights = stacked.at[pl.ds(pl.multiple_of(index * width, width), width)]

        @pl.loop(0, rows // tile)
        def _(i):
            here = pl.ds(pl.multiple_of(i * tile, tile), tile)
            wide = ref[here, :].astype(f32)
            scaled = (wide * gain[pl.ds(index, 1), :]).astype(bf16)
            total = jnp.dot(scaled, weights[...], preferred_element_type=f32)
            square = wide * wide
            square = square[:, : width // 2] + square[:, width // 2 :]
            if first:
                acc[here, :] = total
                squares[here, :] = square
            else:
                acc[here, :] += total
                squares[here, :] += square

    def gathered(dx, other=False):
        index = net.index(dx, other)
        piece(whole.at[index], index)

    piece(tok, net.index(0), first=True)
    net.arrived(2)
    gathered(0, True)
    net.relay_near()
    gathered(-1)
    gathered(1)
    net.arrived(5)
    gathered(-1, True)
    net.arrived(6)
    gathered(1, True)
    net.relay_far()
    gathered(2)
    net.arrived(7)
    net.arrived(8)
    gathered(2, True)

    model_width = width * RING * CORES

    @pl.loop(0, rows // tile)
    def _(i):
        here = pl.ds(pl.multiple_of(i * tile, tile), tile)
        scale = lax.rsqrt(jnp.sum(squares[here, :], axis=1, keepdims=True) / model_width + epsilon)
        projected = [
            (acc[here, pl.ds(local * k, local)] * scale).astype(bf16).astype(f32) for k in range(5)
        ]
        conv_a, conv_gate, query, key, value = projected
        padded[pl.ds(pl.multiple_of(32 + i * tile, 32), tile), :] = conv_a * jax.nn.sigmoid(conv_gate)
        low = left_lanes(query.shape)
        qs[0, here, :] = jnp.where(low, query, 0.0).astype(bf16)
        qs[1, here, :] = jnp.where(low, swap_halves(query), 0.0).astype(bf16)
        kvs[0, here, :] = jnp.where(low, key, swap_halves(value)).astype(bf16)
        kvs[1, here, :] = jnp.where(low, swap_halves(key), value).astype(bf16)

    tail[...] = padded[rows : rows + 32, :]
    shifts = shift[...].astype(f32)
    for head in range(2):
        lines = [shifts[head : head + 1, 128 * k : 128 * (k + 1)] for k in range(rows // 128)]
        lines.append(jnp.zeros((SHIFT_ROWS - len(lines), 128), f32))
        kvs[head, rows : rows + SHIFT_ROWS, :] = jnp.concatenate(lines, axis=0).astype(bf16)
    halo_copy = remote(tail, halo, halo_send, halo_recv, later)
    halo_copy.start()
    net.sent()
    halo_copy.wait()
    padded[0:32, :] = jnp.where(sp == 0, 0.0, halo[...])
    group = net.index(0)
    reach = taps.shape[0]
    tap_values = taps[:, pl.ds(pl.multiple_of(group * local, local), local)].astype(f32)
    step = 64

    @pl.loop(0, rows // step)
    def _(i):
        window = padded[pl.ds(pl.multiple_of(i * step, step), step + 32), :]
        total = jnp.zeros((step, local), f32)
        for rest in range(8):
            turned = window if rest == 0 else window[rest : rest + step + 24]
            for offset in range(rest, 33, 8):
                tap = offset - (33 - reach)
                if tap >= 0:
                    at = offset - rest
                    total = total + tap_values[tap : tap + 1, :] * turned[at : at + step]
        conv_out[pl.ds(pl.multiple_of(i * step, step), step), :] = total


def attention_kernel(
    kvs, qs, conv_own,
    attn_own, conv_all,
    kv_all, queries, sums, behinds, packed, returned,
    kv_send, kv_recv, q_send, q_recv, up_send, up_recv, down_send, down_recv,
    up_pass, up_passed, down_pass, down_passed, o_send, o_recv, x_send, x_recv,
):
    sp, x, c = position()
    z, y = sp // BLOCKS, lax.rem(sp, BLOCKS)
    rows = conv_own.shape[0]
    mirror = PLANES - 1 - z

    def at(plane, column, core):
        return (plane * BLOCKS + column, x, core)

    above, below = lax.rem(z + 1, PLANES), lax.rem(z + PLANES - 1, PLANES)
    partner = at(z, y, 1 - c)
    net = RowGather(conv_own, conv_all, x_send, x_recv)
    peers = [net.right, net.left, at(above, y, c), at(below, y, c)]
    for dy in range(BLOCKS):
        for dc in range(CORES):
            if dy or dc:
                peers.append(at(z, lax.rem(y + dy, BLOCKS), lax.rem(c + dc, CORES)))
            peers.append(at(mirror, dy, dc))
    greet(peers)

    def deliver(src, dst, send, recv, device, mine):
        @pl.when(mine)
        def _():
            pltpu.make_async_copy(src, dst, recv).start()

        @pl.when(jnp.logical_not(mine))
        def _():
            remote(src, dst, send, recv, device).start()

    def delivered(src, dst, send, recv, device, mine):
        @pl.when(jnp.logical_not(mine))
        def _():
            remote(src, dst, send, recv, device).wait_send()

    shipments = []
    for j in range(2):
        head = CORES * c + j
        for core in range(CORES):
            shipments.append((
                kvs.at[j], kv_all.at[z, y], kv_send.at[CORES * j + core], kv_recv.at[y],
                at(z, head, core), jnp.logical_and(head == y, c == core),
            ))
    q_plane = jnp.where(y < 2, z, mirror)
    q_core = jnp.where(jnp.logical_or(y == 0, y == BLOCKS - 1), 0, 1)
    q_slot = jnp.where(y < 2, 0, 1)
    for j in range(2):
        head = CORES * c + j
        shipments.append((
            qs.at[j], queries.at[q_slot], q_send.at[j], q_recv.at[q_slot],
            at(q_plane, head, q_core),
            jnp.logical_and(jnp.logical_and(y < 2, head == y), q_core == c),
        ))
    for shipment in shipments:
        deliver(*shipment)
    net.start()
    conv_all[net.index(0)] = conv_own[...]

    def landed(ref, sem):
        pltpu.make_async_copy(ref, ref, sem).wait()

    for block in range(BLOCKS):
        landed(kv_all.at[z, block], kv_recv.at[block])

    def half(plane):
        return kv_all.at[plane, pl.ds(CORES * c, CORES)]

    def other_half(plane):
        return kv_all.at[plane, pl.ds(CORES * (1 - c), CORES)]

    def up(step):
        plane = lax.rem(z - step + PLANES, PLANES)
        return remote(half(plane), half(plane), up_send.at[step], up_recv.at[step], at(above, y, c))

    def down(step):
        plane = lax.rem(z + step, PLANES)
        return remote(half(plane), half(plane), down_send.at[step], down_recv.at[step], at(below, y, c))

    def pass_up(step):
        plane = lax.rem(z - 1 - step + PLANES, PLANES)
        return remote(half(plane), half(plane), up_pass.at[step], up_passed.at[step], partner)

    def pass_down(step):
        plane = lax.rem(z + 1 + step, PLANES)
        return remote(half(plane), half(plane), down_pass.at[step], down_passed.at[step], partner)

    up(0).start()
    down(0).start()
    for slot in range(2):
        landed(queries.at[slot], q_recv.at[slot])

    row = lax.broadcasted_iota(jnp.int32, (256, 256), 0)
    column = lax.broadcasted_iota(jnp.int32, (256, 256), 1)
    later = jnp.where(row > column, 1.0, 0.0).astype(bf16)

    def block_step(which, plane, block, masked):
        shift_lines = kv_all[plane, block, rows : rows + SHIFT_ROWS, :].astype(f32)
        query = queries[which]
        for part in (1, 0):
            kv = kv_all[plane, block, 256 * part : 256 * (part + 1), :]
            shift = jnp.concatenate(
                [shift_lines[2 * part : 2 * part + 1], shift_lines[2 * part + 1 : 2 * part + 2]], axis=1
            )
            product = lax.dot_general(query, kv, (((1,), (1,)), ((), ())), preferred_element_type=f32)
            score = product * HEAD ** (-0.5) + shift
            fail = jnp.maximum(score, jnp.log(1.0 + jnp.exp(jnp.minimum(score, 80.0))))
            taken = score - fail
            if masked:
                query_row = lax.broadcasted_iota(jnp.int32, score.shape, 0)
                key_row = lax.broadcasted_iota(jnp.int32, score.shape, 1) + 256 * part
                allowed = key_row < query_row
                fail = jnp.where(allowed, fail, 0.0)
            rounded = fail.astype(bf16)
            between = jnp.dot(rounded, later, preferred_element_type=f32)
            behind = behinds[which, plane]
            weight = jnp.exp(taken - (between + jnp.concatenate([behind, behind], axis=1)))
            if masked:
                weight = jnp.where(allowed, weight, 0.0)
            sums[which, plane] += jnp.dot(weight.astype(bf16), kv, preferred_element_type=f32)
            total = between[:, 0:1] + rounded[:, 0:1].astype(f32)
            behinds[which, plane] = behind + jnp.broadcast_to(total, behind.shape)

    def attend(plane):
        @pl.loop(0, 2)
        def _(which):
            last = jnp.where(which == 0, z, mirror)
            block = jnp.where(which == 0, c, BLOCKS - 1 - c)

            @pl.when(plane <= last)
            def _():
                sums[which, plane] = jnp.zeros((rows, 128), f32)
                behinds[which, plane] = jnp.zeros((rows, 128), f32)

                @pl.when(plane == last)
                def _():
                    block_step(which, plane, block, True)

                first = jnp.where(plane == last, block, BLOCKS)

                @pl.loop(0, first)
                def _(i):
                    block_step(which, plane, first - 1 - i, False)

    up_steps, down_steps = PLANES // 2, PLANES // 2 - 1

    @pl.loop(0, up_steps + 1)
    def _(s):
        @pl.when(s > 0)
        def _():
            plane = lax.rem(z - s + PLANES, PLANES)
            landed(half(plane), up_recv.at[s - 1])

            @pl.when(s < up_steps)
            def _():
                up(s).start()

            pass_up(s - 1).start()

            @pl.when(s <= down_steps)
            def _():
                plane = lax.rem(z + s, PLANES)
                landed(half(plane), down_recv.at[s - 1])

                @pl.when(s < down_steps)
                def _():
                    down(s).start()

                pass_down(s - 1).start()

            landed(other_half(plane), up_passed.at[s - 1])

            @pl.when(s <= down_steps)
            def _():
                landed(other_half(lax.rem(z + s, PLANES)), down_passed.at[s - 1])

        @pl.when(s == 1)
        def _():
            net.relay_near()

        @pl.when(s == 2)
        def _():
            net.relay_far()

        @pl.loop(0, 2)
        def _(way):
            @pl.when(jnp.logical_or(way == 0, jnp.logical_and(s > 0, s <= down_steps)))
            def _():
                attend(lax.rem(jnp.where(way == 0, z - s, z + s) + PLANES, PLANES))

    for which in range(2):
        last = z if which == 0 else mirror

        @pl.loop(0, last)
        def _(i):
            plane = last - 1 - i
            behind = behinds[which, last]
            sums[which, last] += jnp.exp(-behind) * sums[which, plane]
            behinds[which, last] = behind + behinds[which, plane]

        done = sums[which, last]
        top, bottom = done[: rows // 2], done[rows // 2 :]
        packed[which] = jnp.where(left_lanes(top.shape), swap_halves(top), bottom).astype(bf16)

    for k in (2, 5, 6, 7, 8):
        net.arrived(k)
    net.sent()
    j = lax.rem(y, CORES)
    returns = []
    for which in range(2):
        owner = at(z, c, y // CORES) if which == 0 else at(mirror, BLOCKS - 1 - c, y // CORES)
        mine = jnp.logical_and(c == y, y // CORES == c) if which == 0 else None
        returns.append((packed.at[which], returned.at[j], o_send.at[which], o_recv.at[j], owner, mine))
    deliver(*returns[0])
    remote(*returns[1][:5]).start()
    for step in range(up_steps):
        up(step).wait_send()
        pass_up(step).wait_send()
    for step in range(down_steps):
        down(step).wait_send()
        pass_down(step).wait_send()
    for shipment in shipments:
        delivered(*shipment)
    for slot in range(2):
        landed(returned.at[slot], o_recv.at[slot])
    first, second = returned[0].astype(f32), returned[1].astype(f32)
    low = left_lanes(first.shape)
    attn_own[: rows // 2, :] = jnp.where(low, first, swap_halves(second)).astype(bf16)
    attn_own[rows // 2 :, :] = jnp.where(low, swap_halves(first), second).astype(bf16)
    delivered(*returns[0])
    remote(*returns[1][:5]).wait_send()


def mix_kernel(
    attn_own, conv_all, norm_gain, conv_gain, attn_gain, weights, mixed,
    whole, scaled, acc, squares, send, recv,
):
    rows, local = attn_own.shape
    pieces = conv_all.shape[0]
    channels = pieces * local
    net = RowGather(attn_own, whole, send, recv)
    greet([net.right, net.left, net.partner])
    net.start()
    tile = 64

    @pl.loop(0, rows // tile)
    def _(i):
        here = pl.ds(pl.multiple_of(i * tile, tile), tile)
        values = [conv_all[p, here, :] for p in range(pieces)]
        total = sum(values[1:], values[0])
        mean = jnp.sum(total, axis=1, keepdims=True) / channels
        centered = [v - mean for v in values]
        square = sum([v * v for v in centered[1:]], centered[0] * centered[0])
        spread = jnp.sum(square, axis=1, keepdims=True) / channels
        inverse = lax.rsqrt(spread + epsilon)
        power = jnp.zeros((tile, local), f32)
        for p in range(pieces):
            normed = centered[p] * inverse * norm_gain[p : p + 1, :]
            kept = (normed * jax.nn.sigmoid(normed)).astype(bf16).astype(f32)
            power = power + kept * kept
            scaled[here, local * p : local * (p + 1)] = (kept * conv_gain[p : p + 1, :]).astype(bf16)
        scale = lax.rsqrt(jnp.sum(power, axis=1, keepdims=True) / channels + epsilon)
        product = jnp.dot(scaled[here, :], weights[:channels, :], preferred_element_type=f32)
        acc[here, :] = product * scale

    def piece(ref, index, first=False):
        wide = ref[...].astype(f32)
        lanes = pl.ds(pl.multiple_of(index * local, local), local)
        scaled[:, lanes] = (wide * attn_gain[pl.ds(index, 1), :]).astype(bf16)
        if first:
            squares[...] = wide * wide
        else:
            squares[...] += wide * wide

    def gathered(dx, other=False):
        index = net.index(dx, other)
        piece(whole.at[index], index)

    piece(attn_own, net.index(0), first=True)
    net.arrived(2)
    gathered(0, True)
    net.relay_near()
    gathered(-1)
    gathered(1)
    net.arrived(5)
    gathered(-1, True)
    net.arrived(6)
    gathered(1, True)
    net.relay_far()
    gathered(2)
    net.arrived(7)
    net.arrived(8)
    gathered(2, True)
    net.sent()

    tile = 128

    @pl.loop(0, rows // tile)
    def _(i):
        here = pl.ds(pl.multiple_of(i * tile, tile), tile)
        scale = lax.rsqrt(jnp.sum(squares[here, :], axis=1, keepdims=True) / channels + epsilon)
        product = jnp.dot(scaled[here, :], weights[channels:, :], preferred_element_type=f32)
        mixed[here, :] = (acc[here, :] + product * scale).astype(bf16)


def in_vmem(count):
    return [pl.BlockSpec(memory_space=VMEM)] * count


def params(collective_id):
    return pltpu.CompilerParams(
        collective_id=collective_id, has_side_effects=True, vmem_limit_bytes=60 * 2**20
    )


def dma(*shape):
    return pltpu.SemaphoreType.DMA(shape)


def per_device(
    tokens, in_gain, conv_a_weight, conv_gate_weight, query_weight, key_weight, value_weight,
    conv_taps, conv_norm_gain, break_shift, conv_out_gain, attn_out_gain, out_weight,
):
    rows, width = tokens.shape
    local = conv_a_weight.shape[1]
    pieces = RING * CORES
    steps = RowGather.steps
    deep = rows + SHIFT_ROWS
    conv_own, kvs, qs = pl.pallas_call(
        project_kernel,
        name="project",
        out_shape=(
            jax.ShapeDtypeStruct((rows, local), f32),
            jax.ShapeDtypeStruct((2, deep, 128), bf16),
            jax.ShapeDtypeStruct((2, rows, 128), bf16),
        ),
        in_specs=in_vmem(4) + [pl.BlockSpec(memory_space=pl.ANY)] * 5,
        out_specs=tuple(in_vmem(3)),
        scratch_shapes=[
            VMEM((pieces, rows, width), bf16),
            VMEM((pieces * width, 5 * local), bf16),
            VMEM((rows, 5 * local), f32),
            VMEM((rows, local), f32),
            VMEM((rows + 32, local), f32),
            VMEM((32, local), f32),
            VMEM((32, local), f32),
            dma(5),
            dma(steps),
            dma(steps),
            pltpu.SemaphoreType.DMA,
            pltpu.SemaphoreType.DMA,
        ],
        compiler_params=params(0),
    )(
        tokens, in_gain.reshape(pieces, width), break_shift, conv_taps,
        conv_a_weight, conv_gate_weight, query_weight, key_weight, value_weight,
    )
    attn_own, conv_all = pl.pallas_call(
        attention_kernel,
        name="attention",
        out_shape=(
            jax.ShapeDtypeStruct((rows, local), bf16),
            jax.ShapeDtypeStruct((pieces, rows, local), f32),
        ),
        in_specs=in_vmem(3),
        out_specs=tuple(in_vmem(2)),
        scratch_shapes=[
            VMEM((PLANES, BLOCKS, deep, 128), bf16),
            VMEM((2, rows, 128), bf16),
            VMEM((2, PLANES, rows, 128), f32),
            VMEM((2, PLANES, rows, 128), f32),
            VMEM((2, rows // 2, 128), bf16),
            VMEM((2, rows // 2, 128), bf16),
            dma(4), dma(4), dma(2), dma(2), dma(4), dma(4), dma(3), dma(3),
            dma(4), dma(4), dma(3), dma(3), dma(2), dma(2), dma(steps), dma(steps),
        ],
        compiler_params=params(1),
    )(kvs, qs, conv_own)
    return pl.pallas_call(
        mix_kernel,
        name="mix",
        out_shape=jax.ShapeDtypeStruct((rows, out_weight.shape[1]), bf16),
        in_specs=in_vmem(6),
        out_specs=pl.BlockSpec(memory_space=VMEM),
        scratch_shapes=[
            VMEM((pieces, rows, local), bf16),
            VMEM((rows, pieces * local), bf16),
            VMEM((rows, out_weight.shape[1]), f32),
            VMEM((rows, local), f32),
            dma(steps),
            dma(steps),
        ],
        compiler_params=params(2),
    )(
        attn_own, conv_all, conv_norm_gain.reshape(pieces, local), conv_out_gain.reshape(pieces, local),
        attn_out_gain.reshape(pieces, local), out_weight,
    )


def solution(mesh):
    columns = P(None, ("fs", "tp"))
    return jax.shard_map(
        per_device,
        mesh=mesh,
        in_specs=(
            P("sp", ("fs", "tp")), P(), columns, columns, columns, columns, columns,
            P(), P(), P(("fs", "tp"), "sp"), P(), P(), columns,
        ),
        out_specs=P("sp", ("fs", "tp")),
        check_vma=False,
    )
```

```python
import jax
import jax.numpy as jnp
from jax import lax
from jax.experimental import pallas as pl
from jax.experimental.pallas import tpu as pltpu
from jax.sharding import PartitionSpec as P

MESH = pl.DeviceIdType.MESH
VMEM = pltpu.VMEM
HEAD = 64
PLANES, BLOCKS, RING, CORES = 8, 4, 4, 2
LOG2E = 1.4426950408889634
MESSAGES = 7
SHIFT_ROWS = 16
epsilon = 1e-06
f32, bf16 = jnp.float32, jnp.bfloat16


def position():
    return lax.axis_index("sp"), lax.axis_index("fs"), lax.axis_index("tp")


def greet(devices):
    barrier = pltpu.get_barrier_semaphore()
    for device in devices:
        pl.semaphore_signal(barrier, inc=1, device_id=device, device_id_type=MESH)
    pl.semaphore_wait(barrier, len(devices))


def remote(src, dst, send, recv, device):
    return pltpu.make_async_remote_copy(
        src_ref=src, dst_ref=dst, send_sem=send, recv_sem=recv, device_id=device, device_id_type=MESH
    )


def left_lanes(shape):
    return lax.broadcasted_iota(jnp.int32, shape, 1) < HEAD


def swap_halves(x):
    return pltpu.roll(x, HEAD, 1)


class RowGather:
    steps = 11

    def __init__(self, own, whole, send, recv):
        self.own, self.whole, self.send, self.recv = own, whole, send, recv
        sp, x, c = position()
        self.x, self.c = x, c
        self.right = (sp, lax.rem(x + 1, RING), c)
        self.left = (sp, lax.rem(x + RING - 1, RING), c)
        self.partner = (sp, x, 1 - c)
        self.half = own.shape[0] // 2

    def index(self, dx, other=False):
        return CORES * lax.rem(self.x + dx + RING, RING) + (1 - self.c if other else self.c)

    def slot(self, dx, other=False, part=None):
        return self.part(self.whole.at[self.index(dx, other)], part)

    def part(self, ref, part):
        return ref if part is None else ref.at[pl.ds(part * self.half, self.half)]

    def out(self, k):
        near = {0: (0, self.right), 1: (1, self.right), 2: (1, self.left), 3: (0, self.left), 4: (None, self.partner)}
        if k in near:
            part, device = near[k]
            src, dst = self.part(self.own, part), self.slot(0, part=part)
        else:
            dx, part, device = {
                5: (-1, 0, self.right),
                6: (1, 1, self.left),
                7: (-1, None, self.partner),
                8: (1, None, self.partner),
                9: (2, 0, self.partner),
                10: (2, 1, self.partner),
            }[k]
            src = dst = self.slot(dx, part=part)
        return remote(src, dst, self.send.at[k], self.recv.at[k], device)

    def arrived(self, *which):
        slots = (
            (-1, False, 0), (-1, False, 1), (1, False, 1), (1, False, 0), (0, True, None), (2, False, 0), (2, False, 1),
            (-1, True, None), (1, True, None), (2, True, 0), (2, True, 1),
        )
        for k in which:
            slot = self.slot(*slots[k])
            remote(slot, slot, self.send.at[k], self.recv.at[k], self.partner).wait_recv()

    def put(self, *which):
        for k in which:
            self.out(k).start()

    def start(self):
        self.put(0, 2, 1, 3, 4)

    def relay_first(self):
        self.arrived(0)
        self.put(5)
        self.arrived(2)
        self.put(6)

    def relay_near(self):
        self.arrived(1)
        self.put(7)
        self.arrived(3)
        self.put(8)

    def relay_far(self):
        self.arrived(5)
        self.put(9)
        self.arrived(6)
        self.put(10)

    def sent(self):
        for k in range(self.steps):
            self.out(k).wait_send()


def landed(ref, sem):
    pltpu.make_async_copy(ref, ref, sem).wait()


def layer_kernel(
    tok, gain, shift, taps, norm_gain, conv_gain, attn_gain, wa, wg, wq, wk, wv, wo,
    mixed,
    tokens_all, stacked, out_weights, acc, squares, padded, tail, halo, kvs, qs, conv_own, conv_all,
    kv_all, q_in, queries, sums, behinds, taken_a, taken_b, fail_a, fail_b, weight_a, weight_b,
    packed, returned, attn_own, attn_all, scaled, total,
    weight_sem, t_send, t_recv, h_send, h_recv, kv_send, kv_recv, pass_send, pass_recv, q_send, q_recv,
    up_send, up_recv, down_send, down_recv, up_pass, up_passed, down_pass, down_passed,
    o_send, o_recv, c_send, c_recv, a_send, a_recv,
):
    sp, x, c = position()
    count = lax.axis_size("sp")
    z, y = sp // BLOCKS, lax.rem(sp, BLOCKS)
    mirror = PLANES - 1 - z
    rows, width = tok.shape
    local = wa.shape[1]
    pieces = RING * CORES
    channels = pieces * local
    model_width = pieces * width

    def at(plane, column, core):
        return (plane * BLOCKS + column, x, core)

    loads = [
        pltpu.make_async_copy(w, stacked.at[:, pl.ds(local * i, local)], weight_sem.at[i])
        for i, w in enumerate((wa, wg, wq, wk, wv))
    ]
    loads.append(pltpu.make_async_copy(wo, out_weights, weight_sem.at[5]))
    for load in loads:
        load.start()

    above, below = lax.rem(z + 1, PLANES), lax.rem(z + PLANES - 1, PLANES)
    partner = at(z, y, 1 - c)
    later_rows = (lax.rem(sp + 1, count), x, c)
    earlier_rows = (lax.rem(sp + count - 1, count), x, c)
    net = RowGather(tok, tokens_all, t_send, t_recv)
    conv_net = RowGather(conv_own, conv_all, c_send, c_recv)
    attn_net = RowGather(attn_own, attn_all, a_send, a_recv)
    peers = [net.right, net.left, at(above, y, c), at(below, y, c), later_rows, earlier_rows]
    for dy in range(BLOCKS):
        for dc in range(CORES):
            if dy or dc:
                peers.append(at(z, lax.rem(y + dy, BLOCKS), lax.rem(c + dc, CORES)))
            peers.append(at(mirror, dy, dc))
    greet(peers)

    net.start()
    shifts = shift[...].astype(f32)
    for head in range(2):
        lines = [shifts[head : head + 1, 128 * k : 128 * (k + 1)] for k in range(rows // 128)]
        lines.append(jnp.zeros((SHIFT_ROWS - len(lines), 128), f32))
        kvs[head, rows : rows + SHIFT_ROWS, :] = jnp.concatenate(lines, axis=0).astype(bf16)
    for load in loads[:5]:
        load.wait()
    tile = 128

    def project(ref, index, first=False):
        weights = stacked.at[pl.ds(pl.multiple_of(index * width, width), width)]
        lines = gain[pl.ds(2 * index, 2), :]
        factor = jnp.concatenate([lines[0:1], lines[1:2]], axis=1)

        @pl.loop(0, rows // tile)
        def _(i):
            here = pl.ds(pl.multiple_of(i * tile, tile), tile)
            wide = ref[here, :].astype(f32)
            product = jnp.dot((wide * factor).astype(bf16), weights[...], preferred_element_type=f32)
            square = wide * wide
            square = square[:, : width // 2] + square[:, width // 2 :]
            if first:
                acc[here, :] = product
                squares[here, :] = square
            else:
                acc[here, :] += product
                squares[here, :] += square

    def project_slot(dx, other=False):
        index = net.index(dx, other)
        project(tokens_all.at[index], index)

    project(tok, net.index(0), first=True)
    net.arrived(4)
    project_slot(0, True)
    net.relay_first()
    net.relay_near()
    project_slot(-1)
    project_slot(1)
    net.arrived(7)
    project_slot(-1, True)
    net.arrived(8)
    project_slot(1, True)
    net.relay_far()
    project_slot(2)
    net.arrived(9, 10)
    project_slot(2, True)

    @pl.loop(0, rows // 2 // tile)
    def _(i):
        top = pl.ds(pl.multiple_of(i * tile, tile), tile)
        bottom = pl.ds(pl.multiple_of(rows // 2 + i * tile, tile), tile)
        query_halves = []
        for here in (top, bottom):
            scale = lax.rsqrt(jnp.sum(squares[here, :], axis=1, keepdims=True) / model_width + epsilon)
            conv_a, conv_gate, query, key, value = [
                (acc[here, pl.ds(local * k, local)] * scale).astype(bf16).astype(f32) for k in range(5)
            ]
            low = left_lanes(query.shape)
            query_halves.append(query)
            kvs[0, here, :] = jnp.where(low, key, swap_halves(value)).astype(bf16)
            kvs[1, here, :] = jnp.where(low, swap_halves(key), value).astype(bf16)
            inside = pl.ds(pl.multiple_of(32 + here.start, 32), tile)
            padded[inside, :] = conv_a * jax.nn.sigmoid(conv_gate)
        first, second = query_halves
        qs[0, top, :] = jnp.where(low, first, swap_halves(second)).astype(bf16)
        qs[1, top, :] = jnp.where(low, swap_halves(first), second).astype(bf16)

    tail[...] = padded[rows : rows + 32, :]

    def deliver(src, dst, send, recv, device, mine):
        @pl.when(mine)
        def _():
            pltpu.make_async_copy(src, dst, recv).start()

        @pl.when(jnp.logical_not(mine))
        def _():
            remote(src, dst, send, recv, device).start()

    def delivered(src, dst, send, recv, device, mine):
        @pl.when(jnp.logical_not(mine))
        def _():
            remote(src, dst, send, recv, device).wait_send()

    shipments = []
    for j in range(2):
        head = CORES * c + j
        shipments.append((
            kvs.at[j], kv_all.at[z, y], kv_send.at[j], kv_recv.at[lax.rem(y, CORES)],
            at(z, head, y // CORES), jnp.logical_and(head == y, y // CORES == c),
        ))
    q_plane = jnp.where(y < 2, z, mirror)
    q_core = jnp.where(jnp.logical_or(y == 0, y == BLOCKS - 1), 0, 1)
    q_slot = jnp.where(y < 2, 0, 1)
    for j in range(2):
        head = CORES * c + j
        shipments.append((
            qs.at[j], q_in.at[q_slot], q_send.at[j], q_recv.at[q_slot],
            at(q_plane, head, q_core),
            jnp.logical_and(jnp.logical_and(y < 2, head == y), q_core == c),
        ))
    for shipment in shipments:
        deliver(*shipment)
    halo_copy = remote(tail, halo, h_send, h_recv, later_rows)
    halo_copy.start()

    halo_copy.wait_recv()
    padded[0:32, :] = jnp.where(sp == 0, 0.0, halo[...])
    reach = taps.shape[0]
    tap_values = taps[:, pl.ds(pl.multiple_of(net.index(0) * local, local), local)].astype(f32)
    step = 64

    @pl.loop(0, rows // step)
    def _(i):
        window = padded[pl.ds(pl.multiple_of(i * step, step), step + 32), :]
        value = jnp.zeros((step, local), f32)
        for rest in range(8):
            turned = window if rest == 0 else window[rest : rest + step + 24]
            for offset in range(rest, 33, 8):
                tap = offset - (33 - reach)
                if tap >= 0:
                    start = offset - rest
                    value = value + tap_values[tap : tap + 1, :] * turned[start : start + step]
        here = pl.ds(pl.multiple_of(i * step, step), step)
        conv_own[here, :] = value
        conv_all[net.index(0), here, :] = value

    def ring_block(plane, parity):
        return kv_all.at[plane, CORES * c + parity]

    def passed_block(plane, parity):
        return kv_all.at[plane, CORES * (1 - c) + parity]

    def up_plane(k):
        return lax.rem(z - k + PLANES, PLANES)

    def down_plane(k):
        return lax.rem(z + k, PLANES)

    def up(m):
        block = ring_block(up_plane(m // 2), lax.rem(m, 2))
        return remote(block, block, up_send.at[m], up_recv.at[m], at(above, y, c))

    def down(m):
        block = ring_block(down_plane(m // 2), 1 - lax.rem(m, 2))
        return remote(block, block, down_send.at[m], down_recv.at[m], at(below, y, c))

    def pass_up(e):
        block = ring_block(up_plane(e // 2 + 1), lax.rem(e, 2))
        return remote(block, block, up_pass.at[e], up_passed.at[e], partner)

    def pass_down(e):
        block = ring_block(down_plane(e // 2 + 1), 1 - lax.rem(e, 2))
        return remote(block, block, down_pass.at[e], down_passed.at[e], partner)

    def pass_own(parity):
        block = ring_block(z, parity)
        return remote(block, block, pass_send.at[parity], pass_recv.at[parity], partner)

    landed(ring_block(z, 0), kv_recv.at[0])
    up(0).start()
    pass_own(0).start()
    landed(ring_block(z, 1), kv_recv.at[1])
    down(0).start()
    up(1).start()
    down(1).start()
    pass_own(1).start()
    conv_net.start()

    for which in range(2):
        @pl.loop(0, PLANES)
        def _(plane):
            sums[which, plane] = jnp.zeros((rows, 128), f32)
            behinds[which, plane] = jnp.zeros((rows, 128), f32)

        landed(q_in.at[which], q_recv.at[which])
        line = q_in[which].astype(f32)
        low = left_lanes(line.shape)
        queries[which, : rows // 2, :] = jnp.where(low, line, 0.0).astype(bf16)
        queries[which, rows // 2 :, :] = jnp.where(low, swap_halves(line), 0.0).astype(bf16)

    for parity in range(2):
        landed(passed_block(z, parity), pass_recv.at[parity])

    def event(e):
        landed(ring_block(up_plane(e // 2 + 1), lax.rem(e, 2)), up_recv.at[e])

        @pl.when(e + 2 < MESSAGES)
        def _():
            up(e + 2).start()

        pass_up(e).start()
        landed(ring_block(down_plane(e // 2 + 1), 1 - lax.rem(e, 2)), down_recv.at[e])

        @pl.when(e + 2 < MESSAGES)
        def _():
            down(e + 2).start()

        pass_down(e).start()
        for turn, relay in ((1, conv_net.relay_first), (2, conv_net.relay_near), (4, conv_net.relay_far)):
            pl.when(e == turn)(relay)

    def handed(e):
        landed(passed_block(up_plane(e // 2 + 1), lax.rem(e, 2)), up_passed.at[e])
        landed(passed_block(down_plane(e // 2 + 1), 1 - lax.rem(e, 2)), down_passed.at[e])

    row = lax.broadcasted_iota(jnp.int32, (256, 256), 0)
    column = lax.broadcasted_iota(jnp.int32, (256, 256), 1)
    later = jnp.where(row > column, 1.0, 0.0).astype(bf16)
    lasts, diagonals = (z, mirror), (c, BLOCKS - 1 - c)

    def score(which, plane, block, taken, fail, masked=False):
        lines = kv_all[plane, block, rows : rows + SHIFT_ROWS, :].astype(f32) * LOG2E
        line = jnp.concatenate([lines[k : k + 1] for k in range(rows // 128)], axis=1)
        product = lax.dot_general(
            queries[which], kv_all[plane, block, :rows, :], (((1,), (1,)), ((), ())), preferred_element_type=f32
        )
        value = product * (LOG2E * HEAD ** (-0.5)) + line
        lost = jnp.maximum(value, lax.log2(1.0 + jnp.exp2(jnp.minimum(value, 115.0))))
        kept = value - lost
        if masked:
            query_row = lax.broadcasted_iota(jnp.int32, value.shape, 0)
            allowed = lax.broadcasted_iota(jnp.int32, value.shape, 1) < query_row
            lost = jnp.where(allowed, lost, 0.0)
            kept = jnp.where(allowed, kept, -jnp.inf)
        taken[...] = kept
        fail[...] = lost.astype(bf16)

    def weigh(which, plane, taken, fail, weight):
        half = rows // 2
        near = jnp.dot(fail[:, half:], later, preferred_element_type=f32)
        far = jnp.dot(fail[:, :half], later, preferred_element_type=f32)
        behind = behinds[which, plane]
        near_total = near[:, 0:1] + fail[:, half : half + 1].astype(f32)
        far_total = far[:, 0:1] + fail[:, 0:1].astype(f32)
        behind_far = behind + jnp.broadcast_to(near_total, behind.shape)
        behinds[which, plane] = behind_far + jnp.broadcast_to(far_total, behind.shape)
        weight[:, half:] = jnp.exp2(taken[:, half:] - near - jnp.concatenate([behind, behind], axis=1)).astype(bf16)
        weight[:, :half] = jnp.exp2(
            taken[:, :half] - far - jnp.concatenate([behind_far, behind_far], axis=1)
        ).astype(bf16)

    def collect(which, plane, slot, block, weight):
        sums[which, slot] += jnp.dot(weight[...], kv_all[plane, block, :rows, :], preferred_element_type=f32)

    def diagonal(which):
        plane, block = lasts[which], diagonals[which]
        sums[which, PLANES] = jnp.zeros((rows, 128), f32)
        behinds[which, PLANES] = jnp.zeros((rows, 128), f32)
        score(which, plane, block, taken_a, fail_a, masked=True)
        weigh(which, PLANES, taken_a, fail_a, weight_a)
        collect(which, plane, PLANES, block, weight_a)

    segments = []
    for order in range(PLANES):
        k = (order + 1) // 2
        plane = up_plane(k) if order % 2 else down_plane(k)
        for which in range(2):
            whole = jnp.where(plane < lasts[which], BLOCKS, 0)
            segments.append((k, plane, which, jnp.where(plane == lasts[which], diagonals[which], whole)))

    def item(i):
        left, found = i, (jnp.int32(0), z, jnp.int32(0), jnp.int32(0))
        for k, plane, which, blocks in segments:
            inside = jnp.logical_and(left >= 0, left < blocks)
            here = (k, plane, which, blocks - 1 - left)
            found = tuple(jnp.where(inside, new, old) for new, old in zip(here, found))
            left = left - blocks
        return found

    items = (BLOCKS - 1) + BLOCKS * (PLANES - 1)

    def catch_up(done, target, handle):
        lax.fori_loop(done, target, lambda e, _: (handle(e), 0)[1], 0)
        return jnp.maximum(done, target)

    def prepare(i, step_needed, seen, had):
        needed = jnp.minimum(2 * step_needed, MESSAGES)
        expected = jnp.minimum(jnp.maximum(i - 1, 0) // 4, MESSAGES)
        seen = catch_up(seen, jnp.maximum(needed, expected), event)
        had = catch_up(had, needed, handed)
        return seen, had

    diagonal(0)
    zero = jnp.int32(0)
    first, second = item(zero), item(zero + 1)
    seen, had = prepare(zero, second[0], zero, zero)
    score(first[2], first[1], first[3], taken_a, fail_a)
    score(second[2], second[1], second[3], taken_b, fail_b)
    weigh(first[2], first[1], taken_a, fail_a, weight_a)

    def stages(now, after, coming, taken, fail, weight, other_taken, other_fail, other_weight):
        weigh(after[2], after[1], other_taken, other_fail, other_weight)
        score(coming[2], coming[1], coming[3], taken, fail)
        collect(now[2], now[1], now[1], now[3], weight)

    def pair(j, carried):
        now, after, seen, had = carried
        coming, following = item(2 * j + 2), item(2 * j + 3)
        seen, had = prepare(2 * j, jnp.maximum(coming[0], following[0]), seen, had)
        stages(now, after, coming, taken_a, fail_a, weight_a, taken_b, fail_b, weight_b)
        stages(after, coming, following, taken_b, fail_b, weight_b, taken_a, fail_a, weight_a)
        return coming, following, seen, had

    final, _, seen, had = lax.fori_loop(0, (items - 1) // 2, pair, (first, second, seen, had))
    collect(final[2], final[1], final[1], final[3], weight_a)
    seen = catch_up(seen, MESSAGES, event)
    catch_up(had, MESSAGES, handed)
    diagonal(1)

    for which in range(2):
        last = lasts[which]

        @pl.loop(0, last + 1)
        def _(i):
            plane = last - i
            behind = behinds[which, PLANES]
            sums[which, PLANES] += jnp.exp2(-behind) * sums[which, plane]
            behinds[which, PLANES] = behind + behinds[which, plane]

        done = sums[which, PLANES]
        top, bottom = done[: rows // 2], done[rows // 2 :]
        packed[which] = jnp.where(left_lanes(top.shape), swap_halves(top), bottom).astype(bf16)

    j = lax.rem(y, CORES)
    returns = []
    for which in range(2):
        owner = at(z, c, y // CORES) if which == 0 else at(mirror, BLOCKS - 1 - c, y // CORES)
        mine = jnp.logical_and(c == y, y // CORES == c) if which == 0 else None
        returns.append((packed.at[which], returned.at[j], o_send.at[which], o_recv.at[j], owner, mine))
    for e in range(MESSAGES):
        up(e).wait_send()
        pass_up(e).wait_send()
        down(e).wait_send()
        pass_down(e).wait_send()
    deliver(*returns[0])
    remote(*returns[1][:5]).start()
    net.sent()
    halo_copy.wait_send()
    for parity in range(2):
        pass_own(parity).wait_send()
    for shipment in shipments:
        delivered(*shipment)
    for slot in range(2):
        landed(returned.at[slot], o_recv.at[slot])
    first, second = returned[0].astype(f32), returned[1].astype(f32)
    low = left_lanes(first.shape)
    attn_own[: rows // 2, :] = jnp.where(low, first, swap_halves(second)).astype(bf16)
    attn_own[rows // 2 :, :] = jnp.where(low, swap_halves(first), second).astype(bf16)
    delivered(*returns[0])
    remote(*returns[1][:5]).wait_send()

    attn_net.start()
    conv_net.arrived(4, 7, 8, 9, 10)
    conv_net.sent()
    loads[5].wait()

    @pl.loop(0, rows // step)
    def _(i):
        here = pl.ds(pl.multiple_of(i * step, step), step)
        values = [conv_all[p, here, :] for p in range(pieces)]
        mean = jnp.sum(sum(values[1:], values[0]), axis=1, keepdims=True) / channels
        centered = [v - mean for v in values]
        square = sum([v * v for v in centered[1:]], centered[0] * centered[0])
        spread = jnp.sum(square, axis=1, keepdims=True) / channels
        inverse = lax.rsqrt(spread + epsilon)
        power = jnp.zeros((step, local), f32)
        for p in range(pieces):
            normed = centered[p] * inverse * norm_gain[p : p + 1, :]
            kept = (normed * jax.nn.sigmoid(normed)).astype(bf16).astype(f32)
            power = power + kept * kept
            scaled[here, local * p : local * (p + 1)] = (kept * conv_gain[p : p + 1, :]).astype(bf16)
        scale = lax.rsqrt(jnp.sum(power, axis=1, keepdims=True) / channels + epsilon)
        total[here, :] = jnp.dot(scaled[here, :], out_weights[:channels, :], preferred_element_type=f32) * scale

    def rescale(ref, index, first=False):
        wide = ref[...].astype(f32)
        lanes = pl.ds(pl.multiple_of(index * local, local), local)
        scaled[:, lanes] = (wide * attn_gain[pl.ds(index, 1), :]).astype(bf16)
        if first:
            squares[...] = wide * wide
        else:
            squares[...] += wide * wide

    def rescale_slot(dx, other=False):
        index = attn_net.index(dx, other)
        rescale(attn_all.at[index], index)

    rescale(attn_own, attn_net.index(0), first=True)
    attn_net.relay_first()
    attn_net.arrived(4)
    rescale_slot(0, True)
    attn_net.relay_near()
    rescale_slot(-1)
    rescale_slot(1)
    attn_net.arrived(7)
    rescale_slot(-1, True)
    attn_net.arrived(8)
    rescale_slot(1, True)
    attn_net.relay_far()
    rescale_slot(2)
    attn_net.arrived(9, 10)
    rescale_slot(2, True)

    @pl.loop(0, rows // tile)
    def _(i):
        here = pl.ds(pl.multiple_of(i * tile, tile), tile)
        scale = lax.rsqrt(jnp.sum(squares[here, :], axis=1, keepdims=True) / channels + epsilon)
        product = jnp.dot(scaled[here, :], out_weights[channels:, :], preferred_element_type=f32)
        mixed[here, :] = (total[here, :] + product * scale).astype(bf16)

    attn_net.sent()


def dma(*shape):
    return pltpu.SemaphoreType.DMA(shape)


def per_device(
    tokens, in_gain, conv_a_weight, conv_gate_weight, query_weight, key_weight, value_weight,
    conv_taps, conv_norm_gain, break_shift, conv_out_gain, attn_out_gain, out_weight,
):
    rows, width = tokens.shape
    local = conv_a_weight.shape[1]
    out_width = out_weight.shape[1]
    pieces = RING * CORES
    steps = RowGather.steps
    deep = rows + SHIFT_ROWS
    scratch = [
        VMEM((pieces, rows, width), bf16),
        VMEM((pieces * width, 5 * local), bf16),
        VMEM(out_weight.shape, bf16),
        VMEM((rows, 5 * local), f32),
        VMEM((rows, local), f32),
        VMEM((rows + 32, local), f32),
        VMEM((32, local), f32),
        VMEM((32, local), f32),
        VMEM((2, deep, 128), bf16),
        VMEM((2, rows // 2, 128), bf16),
        VMEM((rows, local), f32),
        VMEM((pieces, rows, local), f32),
        VMEM((PLANES, BLOCKS, deep, 128), bf16),
        VMEM((2, rows // 2, 128), bf16),
        VMEM((2, rows, 128), bf16),
        VMEM((2, PLANES + 1, rows, 128), f32),
        VMEM((2, PLANES + 1, rows, 128), f32),
        VMEM((rows, rows), f32),
        VMEM((rows, rows), f32),
        VMEM((rows, rows), bf16),
        VMEM((rows, rows), bf16),
        VMEM((rows, rows), bf16),
        VMEM((rows, rows), bf16),
        VMEM((2, rows // 2, 128), bf16),
        VMEM((2, rows // 2, 128), bf16),
        VMEM((rows, local), bf16),
        VMEM((pieces, rows, local), bf16),
        VMEM((rows, pieces * local), bf16),
        VMEM((rows, out_width), f32),
        dma(6), dma(steps), dma(steps), pltpu.SemaphoreType.DMA, pltpu.SemaphoreType.DMA,
        dma(2), dma(2), dma(2), dma(2), dma(2), dma(2),
        dma(MESSAGES), dma(MESSAGES), dma(MESSAGES), dma(MESSAGES),
        dma(MESSAGES), dma(MESSAGES), dma(MESSAGES), dma(MESSAGES),
        dma(2), dma(2), dma(steps), dma(steps), dma(steps), dma(steps),
    ]
    return pl.pallas_call(
        layer_kernel,
        name="layer",
        out_shape=jax.ShapeDtypeStruct((rows, out_width), bf16),
        in_specs=[pl.BlockSpec(memory_space=VMEM)] * 7 + [pl.BlockSpec(memory_space=pl.ANY)] * 6,
        out_specs=pl.BlockSpec(memory_space=VMEM),
        scratch_shapes=scratch,
        compiler_params=pltpu.CompilerParams(
            collective_id=0, has_side_effects=True, vmem_limit_bytes=60 * 2**20
        ),
    )(
        tokens, in_gain.reshape(2 * pieces, width // 2), break_shift, conv_taps,
        conv_norm_gain.reshape(pieces, local), conv_out_gain.reshape(pieces, local),
        attn_out_gain.reshape(pieces, local),
        conv_a_weight, conv_gate_weight, query_weight, key_weight, value_weight, out_weight,
    )


def solution(mesh):
    columns = P(None, ("fs", "tp"))
    return jax.shard_map(
        per_device,
        mesh=mesh,
        in_specs=(
            P("sp", ("fs", "tp")), P(), columns, columns, columns, columns, columns,
            P(), P(), P(("fs", "tp"), "sp"), P(), P(), columns,
        ),
        out_specs=P("sp", ("fs", "tp")),
        check_vma=False,
    )
```

```python
import jax
import jax.numpy as jnp
from jax import lax
from jax.experimental import pallas as pl
from jax.experimental.pallas import tpu as pltpu
from jax.sharding import PartitionSpec as P

MESH = pl.DeviceIdType.MESH
VMEM = pltpu.VMEM
HEAD = 64
PLANES, BLOCKS, RING, CORES = 8, 4, 4, 2
LOG2E = 1.4426950408889634
MESSAGES, NEAR = 8, 3
HELP = 4
SHIFT_ROWS = 16
epsilon = 1e-06
f32, bf16 = jnp.float32, jnp.bfloat16


def position():
    return lax.axis_index("sp"), lax.axis_index("fs"), lax.axis_index("tp")


def greet(devices):
    barrier = pltpu.get_barrier_semaphore()
    for device in devices:
        pl.semaphore_signal(barrier, inc=1, device_id=device, device_id_type=MESH)
    pl.semaphore_wait(barrier, len(devices))


def remote(src, dst, send, recv, device):
    return pltpu.make_async_remote_copy(
        src_ref=src, dst_ref=dst, send_sem=send, recv_sem=recv, device_id=device, device_id_type=MESH
    )


def left_lanes(shape):
    return lax.broadcasted_iota(jnp.int32, shape, 1) < HEAD


def swap_halves(x):
    return pltpu.roll(x, HEAD, 1)


class RowGather:
    steps = 11

    def __init__(self, own, whole, send, recv):
        self.own, self.whole, self.send, self.recv = own, whole, send, recv
        sp, x, c = position()
        self.x, self.c = x, c
        self.right = (sp, lax.rem(x + 1, RING), c)
        self.left = (sp, lax.rem(x + RING - 1, RING), c)
        self.partner = (sp, x, 1 - c)
        self.half = own.shape[0] // 2

    def index(self, dx, other=False):
        return CORES * lax.rem(self.x + dx + RING, RING) + (1 - self.c if other else self.c)

    def slot(self, dx, other=False, part=None):
        return self.part(self.whole.at[self.index(dx, other)], part)

    def part(self, ref, part):
        return ref if part is None else ref.at[pl.ds(part * self.half, self.half)]

    def out(self, k):
        near = {0: (0, self.right), 1: (1, self.right), 2: (1, self.left), 3: (0, self.left), 4: (None, self.partner)}
        if k in near:
            part, device = near[k]
            src, dst = self.part(self.own, part), self.slot(0, part=part)
        else:
            dx, part, device = {
                5: (-1, 0, self.right),
                6: (1, 1, self.left),
                7: (-1, None, self.partner),
                8: (1, None, self.partner),
                9: (2, 0, self.partner),
                10: (2, 1, self.partner),
            }[k]
            src = dst = self.slot(dx, part=part)
        return remote(src, dst, self.send.at[k], self.recv.at[k], device)

    def arrived(self, *which):
        slots = (
            (-1, False, 0), (-1, False, 1), (1, False, 1), (1, False, 0), (0, True, None), (2, False, 0), (2, False, 1),
            (-1, True, None), (1, True, None), (2, True, 0), (2, True, 1),
        )
        for k in which:
            slot = self.slot(*slots[k])
            remote(slot, slot, self.send.at[k], self.recv.at[k], self.partner).wait_recv()

    def put(self, *which):
        for k in which:
            self.out(k).start()

    def start(self):
        self.put(0, 2, 1, 3, 4)

    def relay_first(self):
        self.arrived(0)
        self.put(5)
        self.arrived(2)
        self.put(6)

    def relay_near(self):
        self.arrived(1)
        self.put(7)
        self.arrived(3)
        self.put(8)

    def relay_far(self):
        self.arrived(5)
        self.put(9)
        self.arrived(6)
        self.put(10)

    def sent(self):
        for k in range(self.steps):
            self.out(k).wait_send()


def landed(ref, sem):
    pltpu.make_async_copy(ref, ref, sem).wait()


def layer_kernel(
    tok, gain, shift, taps, norm_gain, conv_gain, attn_gain, wa, wg, wq, wk, wv, wo,
    mixed,
    tokens_all, stacked, out_weights, acc, squares, padded, tail, halo, kvs, qs, conv_own, conv_all,
    kv_all, q_in, queries, sums, behinds, taken_a, taken_b, fail_a, fail_b, weight_a, weight_b,
    packed, far_packed, far_in, returned, attn_own, attn_all, scaled, total,
    weight_sem, t_send, t_recv, h_send, h_recv, kv_send, kv_recv, pass_send, pass_recv, q_send, q_recv,
    up_send, up_recv, down_send, down_recv, up_pass, up_passed, down_pass, down_passed,
    f_send, f_recv, o_send, o_recv, c_send, c_recv, a_send, a_recv,
):
    sp, x, c = position()
    count = lax.axis_size("sp")
    z, y = sp // BLOCKS, lax.rem(sp, BLOCKS)
    mirror = PLANES - 1 - z
    rows, width = tok.shape
    local = wa.shape[1]
    pieces = RING * CORES
    channels = pieces * local
    model_width = pieces * width

    def at(plane, column, core):
        return (plane * BLOCKS + column, x, core)

    loads = [
        pltpu.make_async_copy(w, stacked.at[:, pl.ds(local * i, local)], weight_sem.at[i])
        for i, w in enumerate((wa, wg, wq, wk, wv))
    ]
    loads.append(pltpu.make_async_copy(wo, out_weights, weight_sem.at[5]))
    for load in loads:
        load.start()

    above, below = lax.rem(z + 1, PLANES), lax.rem(z + PLANES - 1, PLANES)
    partner = at(z, y, 1 - c)
    later_rows = (lax.rem(sp + 1, count), x, c)
    earlier_rows = (lax.rem(sp + count - 1, count), x, c)
    net = RowGather(tok, tokens_all, t_send, t_recv)
    conv_net = RowGather(conv_own, conv_all, c_send, c_recv)
    attn_net = RowGather(attn_own, attn_all, a_send, a_recv)
    peers = [net.right, net.left, at(above, y, c), at(below, y, c), later_rows, earlier_rows]
    for dy in range(BLOCKS):
        for dc in range(CORES):
            if dy or dc:
                peers.append(at(z, lax.rem(y + dy, BLOCKS), lax.rem(c + dc, CORES)))
            peers.append(at(mirror, dy, dc))
    greet(peers)

    net.start()
    shifts = shift[...].astype(f32)
    for head in range(2):
        lines = [shifts[head : head + 1, 128 * k : 128 * (k + 1)] for k in range(rows // 128)]
        lines.append(jnp.zeros((SHIFT_ROWS - len(lines), 128), f32))
        kvs[head, rows : rows + SHIFT_ROWS, :] = jnp.concatenate(lines, axis=0).astype(bf16)
    for load in loads[:5]:
        load.wait()
    tile = 128

    def project(ref, index, first=False):
        weights = stacked.at[pl.ds(pl.multiple_of(index * width, width), width)]
        lines = gain[pl.ds(2 * index, 2), :]
        factor = jnp.concatenate([lines[0:1], lines[1:2]], axis=1)

        @pl.loop(0, rows // tile)
        def _(i):
            here = pl.ds(pl.multiple_of(i * tile, tile), tile)
            wide = ref[here, :].astype(f32)
            product = jnp.dot((wide * factor).astype(bf16), weights[...], preferred_element_type=f32)
            square = wide * wide
            square = square[:, : width // 2] + square[:, width // 2 :]
            if first:
                acc[here, :] = product
                squares[here, :] = square
            else:
                acc[here, :] += product
                squares[here, :] += square

    def project_slot(dx, other=False):
        index = net.index(dx, other)
        project(tokens_all.at[index], index)

    project(tok, net.index(0), first=True)
    net.arrived(4)
    project_slot(0, True)
    net.relay_first()
    net.relay_near()
    project_slot(-1)
    project_slot(1)
    net.arrived(7)
    project_slot(-1, True)
    net.arrived(8)
    project_slot(1, True)
    net.relay_far()
    project_slot(2)
    net.arrived(9, 10)
    project_slot(2, True)

    @pl.loop(0, rows // 2 // tile)
    def _(i):
        top = pl.ds(pl.multiple_of(i * tile, tile), tile)
        bottom = pl.ds(pl.multiple_of(rows // 2 + i * tile, tile), tile)
        query_halves = []
        for here in (top, bottom):
            scale = lax.rsqrt(jnp.sum(squares[here, :], axis=1, keepdims=True) / model_width + epsilon)
            conv_a, conv_gate, query, key, value = [
                (acc[here, pl.ds(local * k, local)] * scale).astype(bf16).astype(f32) for k in range(5)
            ]
            low = left_lanes(query.shape)
            query_halves.append(query)
            kvs[0, here, :] = jnp.where(low, key, swap_halves(value)).astype(bf16)
            kvs[1, here, :] = jnp.where(low, swap_halves(key), value).astype(bf16)
            inside = pl.ds(pl.multiple_of(32 + here.start, 32), tile)
            padded[inside, :] = conv_a * jax.nn.sigmoid(conv_gate)
        first, second = query_halves
        qs[0, top, :] = jnp.where(low, first, swap_halves(second)).astype(bf16)
        qs[1, top, :] = jnp.where(low, swap_halves(first), second).astype(bf16)

    tail[...] = padded[rows : rows + 32, :]

    def deliver(src, dst, send, recv, device, mine):
        @pl.when(mine)
        def _():
            pltpu.make_async_copy(src, dst, recv).start()

        @pl.when(jnp.logical_not(mine))
        def _():
            remote(src, dst, send, recv, device).start()

    def delivered(src, dst, send, recv, device, mine):
        @pl.when(jnp.logical_not(mine))
        def _():
            remote(src, dst, send, recv, device).wait_send()

    shipments = []
    for j in range(2):
        head = CORES * c + j
        shipments.append((
            kvs.at[j], kv_all.at[z, y], kv_send.at[j], kv_recv.at[lax.rem(y, CORES)],
            at(z, head, y // CORES), jnp.logical_and(head == y, y // CORES == c),
        ))
    q_core = jnp.where(jnp.logical_or(y == 0, y == BLOCKS - 1), 0, 1)
    q_slot = jnp.where(y < 2, 0, 1)
    helped, helping = z >= HELP, z < HELP
    far_queries = []
    for j in range(2):
        head = CORES * c + j
        shipments.append((
            qs.at[j], q_in.at[q_slot], q_send.at[j], q_recv.at[q_slot],
            at(z, head, q_core), jnp.logical_and(head == y, q_core == c),
        ))
        far_queries.append(remote(
            qs.at[j], q_in.at[2 + q_slot], q_send.at[2 + j], q_recv.at[2 + q_slot], at(mirror, head, q_core)
        ))
    for shipment in shipments:
        deliver(*shipment)
    halo_copy = remote(tail, halo, h_send, h_recv, later_rows)
    halo_copy.start()

    @pl.when(helped)
    def _():
        for copy in far_queries:
            copy.start()

    halo_copy.wait_recv()
    padded[0:32, :] = jnp.where(sp == 0, 0.0, halo[...])
    reach = taps.shape[0]
    tap_values = taps[:, pl.ds(pl.multiple_of(net.index(0) * local, local), local)].astype(f32)
    step = 64

    @pl.loop(0, rows // step)
    def _(i):
        window = padded[pl.ds(pl.multiple_of(i * step, step), step + 32), :]
        value = jnp.zeros((step, local), f32)
        for rest in range(8):
            turned = window if rest == 0 else window[rest : rest + step + 24]
            for offset in range(rest, 33, 8):
                tap = offset - (33 - reach)
                if tap >= 0:
                    start = offset - rest
                    value = value + tap_values[tap : tap + 1, :] * turned[start : start + step]
        here = pl.ds(pl.multiple_of(i * step, step), step)
        conv_own[here, :] = value
        conv_all[net.index(0), here, :] = value

    def ring_block(plane, parity):
        return kv_all.at[plane, CORES * c + parity]

    def passed_block(plane, parity):
        return kv_all.at[plane, CORES * (1 - c) + parity]

    def up_plane(k):
        return lax.rem(z - k + PLANES, PLANES)

    def down_plane(k):
        return lax.rem(z + k, PLANES)

    def up(m):
        block = ring_block(up_plane(m // 2), lax.rem(m, 2))
        return remote(block, block, up_send.at[m], up_recv.at[m], at(above, y, c))

    def down(m):
        block = ring_block(down_plane(m // 2), 1 - lax.rem(m, 2))
        return remote(block, block, down_send.at[m], down_recv.at[m], at(below, y, c))

    def pass_up(e):
        block = ring_block(up_plane(e // 2 + 1), lax.rem(e, 2))
        return remote(block, block, up_pass.at[e], up_passed.at[e], partner)

    def pass_down(e):
        block = ring_block(down_plane(e // 2 + 1), 1 - lax.rem(e, 2))
        return remote(block, block, down_pass.at[e], down_passed.at[e], partner)

    def pass_own(parity):
        block = ring_block(z, parity)
        return remote(block, block, pass_send.at[parity], pass_recv.at[parity], partner)

    def rises(plane, k, core):
        return jnp.logical_and(plane >= 0, jnp.logical_or(k < NEAR, core == 1))

    def up_goes(m):
        return jnp.logical_and(rises(z - m // 2, m // 2, c), z < PLANES - 1)

    def up_comes(e, core):
        return rises(z - 1 - e // 2, e // 2, core)

    def down_goes(m):
        return jnp.logical_and(jnp.logical_and(z + m // 2 < HELP, m < 2 * NEAR), z > 0)

    def down_comes(e):
        return jnp.logical_and(z + 1 + e // 2 < HELP, e < 2 * NEAR)

    def send_up(m):
        pl.when(up_goes(m))(lambda: up(m).start())

    def send_down(m):
        pl.when(down_goes(m))(lambda: down(m).start())

    for parity in range(2):
        landed(ring_block(z, parity), kv_recv.at[parity])
        send_up(parity)
        pass_own(parity).start()
        if parity == 1:
            send_down(0)
            send_down(1)
    conv_net.start()

    @pl.loop(0, sums.shape[0])
    def _(slot):
        sums[slot] = jnp.zeros((rows, 128), f32)
        behinds[slot] = jnp.zeros((rows, 128), f32)

    def unpack(slot):
        landed(q_in.at[slot], q_recv.at[slot])
        line = q_in[slot].astype(f32)
        low = left_lanes(line.shape)
        queries[slot, : rows // 2, :] = jnp.where(low, line, 0.0).astype(bf16)
        queries[slot, rows // 2 :, :] = jnp.where(low, swap_halves(line), 0.0).astype(bf16)

    unpack(0)
    unpack(1)
    for parity in range(2):
        landed(passed_block(z, parity), pass_recv.at[parity])

    def event(e):
        @pl.when(up_comes(e, c))
        def _():
            landed(ring_block(up_plane(e // 2 + 1), lax.rem(e, 2)), up_recv.at[e])

            @pl.when(e + 2 < MESSAGES)
            def _():
                send_up(e + 2)

            pass_up(e).start()

        @pl.when(down_comes(e))
        def _():
            landed(ring_block(down_plane(e // 2 + 1), 1 - lax.rem(e, 2)), down_recv.at[e])

            @pl.when(e + 2 < 2 * NEAR)
            def _():
                send_down(e + 2)

            pass_down(e).start()

        for turn, relay in ((1, conv_net.relay_first), (2, conv_net.relay_near), (4, conv_net.relay_far)):
            pl.when(e == turn)(relay)

    def handed(e):
        @pl.when(up_comes(e, 1 - c))
        def _():
            landed(passed_block(up_plane(e // 2 + 1), lax.rem(e, 2)), up_passed.at[e])

        @pl.when(down_comes(e))
        def _():
            landed(passed_block(down_plane(e // 2 + 1), 1 - lax.rem(e, 2)), down_passed.at[e])

    row = lax.broadcasted_iota(jnp.int32, (256, 256), 0)
    column = lax.broadcasted_iota(jnp.int32, (256, 256), 1)
    later = jnp.where(row > column, 1.0, 0.0).astype(bf16)

    def score(which, plane, block, taken, fail, masked=False):
        lines = kv_all[plane, block, rows : rows + SHIFT_ROWS, :].astype(f32) * LOG2E
        line = jnp.concatenate([lines[k : k + 1] for k in range(rows // 128)], axis=1)
        product = lax.dot_general(
            queries[which], kv_all[plane, block, :rows, :], (((1,), (1,)), ((), ())), preferred_element_type=f32
        )
        value = product * (LOG2E * HEAD ** (-0.5)) + line
        lost = jnp.maximum(value, lax.log2(1.0 + jnp.exp2(jnp.minimum(value, 115.0))))
        kept = value - lost
        if masked:
            query_row = lax.broadcasted_iota(jnp.int32, value.shape, 0)
            allowed = lax.broadcasted_iota(jnp.int32, value.shape, 1) < query_row
            lost = jnp.where(allowed, lost, 0.0)
            kept = jnp.where(allowed, kept, -jnp.inf)
        taken[...] = kept
        fail[...] = lost.astype(bf16)

    def weigh(slot, taken, fail, weight):
        half = rows // 2
        near = jnp.dot(fail[:, half:], later, preferred_element_type=f32)
        far = jnp.dot(fail[:, :half], later, preferred_element_type=f32)
        behind = behinds[slot]
        near_total = near[:, 0:1] + fail[:, half : half + 1].astype(f32)
        far_total = far[:, 0:1] + fail[:, 0:1].astype(f32)
        behind_far = behind + jnp.broadcast_to(near_total, behind.shape)
        behinds[slot] = behind_far + jnp.broadcast_to(far_total, behind.shape)
        weight[:, half:] = jnp.exp2(taken[:, half:] - near - jnp.concatenate([behind, behind], axis=1)).astype(bf16)
        weight[:, :half] = jnp.exp2(
            taken[:, :half] - far - jnp.concatenate([behind_far, behind_far], axis=1)
        ).astype(bf16)

    def collect(plane, slot, block, weight):
        sums[slot] += jnp.dot(weight[...], kv_all[plane, block, :rows, :], preferred_element_type=f32)

    segments = []
    for k in range(NEAR + 2):
        for kind, plane in ((2, z - k), (2, z + k), (0, z - k)):
            if kind and (k > NEAR or (k == 0 and segments)):
                continue
            if kind:
                part = jnp.where(plane < HELP - 1 - z, BLOCKS, jnp.where(plane == HELP - 1 - z, BLOCKS // 2, 0))
                blocks = jnp.where(jnp.logical_and(helping, plane >= 0), 2 * part, 0)
            elif k == 0:
                blocks = jnp.int32(BLOCKS - 1)
            else:
                blocks = jnp.where(plane >= 0, 2 * (BLOCKS if k <= NEAR else BLOCKS // 2), 0)
            segments.append((jnp.int32(k), plane, jnp.int32(kind), blocks))

    def item(i):
        left, (k, plane, kind, place) = i, (jnp.int32(0), z, jnp.int32(0), jnp.int32(0))
        for step_k, step_plane, step_kind, blocks in segments:
            inside = jnp.logical_and(left >= 0, left < blocks)
            k = jnp.where(inside, step_k, k)
            plane = jnp.where(inside, step_plane, plane)
            kind = jnp.where(inside, step_kind, kind)
            place = jnp.where(inside, left, place)
            left = left - blocks
        mine, here = kind == 0, plane == z
        part = jnp.where(plane < HELP - 1 - z, BLOCKS, BLOCKS // 2)
        near_count = jnp.where(here, c, jnp.where(k <= NEAR, BLOCKS, BLOCKS // 2))
        first_count = jnp.where(mine, near_count, part)
        first_top = jnp.where(mine, jnp.where(here, c, BLOCKS), part)
        second_top = jnp.where(mine, jnp.where(here, BLOCKS - 1 - c, BLOCKS), part)
        second = place >= first_count
        block = jnp.where(second, second_top - 1 - (place - first_count), first_top - 1 - place)
        which = kind + jnp.where(second, 1, 0)
        slot = jnp.where(mine, which, 2 + HELP * (which - 2) + plane)
        return k, plane, which, block, slot

    items = (BLOCKS - 1) + BLOCKS * (PLANES - 1)
    so_far, help_end = jnp.int32(0), jnp.int32(-BLOCKS)
    for _, _, kind, blocks in segments:
        so_far = so_far + blocks
        help_end = jnp.where(jnp.logical_and(kind == 2, blocks > 0), so_far, help_end)

    far_returns = [
        remote(far_packed.at[w], far_in.at[w], f_send.at[w], f_recv.at[w], at(mirror, y, c)) for w in range(2)
    ]

    def pack(value):
        top, bottom = value[: rows // 2], value[rows // 2 :]
        return jnp.where(left_lanes(top.shape), swap_halves(top), bottom).astype(bf16)

    def return_far():
        for w in range(2):
            base = 2 + HELP * w
            for plane in range(HELP - 2, -1, -1):
                behind = behinds[base + HELP - 1]
                sums[base + HELP - 1] += jnp.exp2(-behind) * sums[base + plane]
                behinds[base + HELP - 1] = behind + behinds[base + plane]
            far_packed[w] = pack(sums[base + HELP - 1])
        for copy in far_returns:
            copy.start()

    def catch_up(done, target, handle):
        lax.fori_loop(done, target, lambda e, _: (handle(e), 0)[1], 0)
        return jnp.maximum(done, target)

    def prepare(i, step_needed, seen, had):
        needed = jnp.minimum(2 * step_needed, MESSAGES)
        expected = jnp.minimum(jnp.maximum(i + 3, 0) // 4, MESSAGES)
        seen = catch_up(seen, jnp.maximum(needed, expected), event)
        had = catch_up(had, needed, handed)
        return seen, had

    @pl.loop(0, 2)
    def _(which):
        block = jnp.where(which == 0, c, BLOCKS - 1 - c)
        score(which, z, block, taken_a, fail_a, masked=True)
        weigh(which, taken_a, fail_a, weight_a)
        collect(z, which, block, weight_a)

    @pl.when(helping)
    def _():
        unpack(2)
        unpack(3)

    zero = jnp.int32(0)
    first, second = item(zero), item(zero + 1)
    seen, had = prepare(zero, second[0], zero, zero)
    score(first[2], first[1], first[3], taken_a, fail_a)
    score(second[2], second[1], second[3], taken_b, fail_b)
    weigh(first[4], taken_a, fail_a, weight_a)

    def stages(now, after, coming, taken, fail, weight, other_taken, other_fail, other_weight):
        weigh(after[4], other_taken, other_fail, other_weight)
        score(coming[2], coming[1], coming[3], taken, fail)
        collect(now[1], now[4], now[3], weight)

    def pair(j, carried):
        now, after, seen, had = carried
        coming, following = item(2 * j + 2), item(2 * j + 3)
        seen, had = prepare(2 * j, jnp.maximum(coming[0], following[0]), seen, had)
        pl.when(jnp.logical_and(help_end > 2 * j - 2, help_end <= 2 * j))(return_far)
        stages(now, after, coming, taken_a, fail_a, weight_a, taken_b, fail_b, weight_b)
        stages(after, coming, following, taken_b, fail_b, weight_b, taken_a, fail_a, weight_a)
        return coming, following, seen, had

    final, _, seen, had = lax.fori_loop(0, (items - 1) // 2, pair, (first, second, seen, had))
    collect(final[1], final[4], final[3], weight_a)
    pl.when(help_end > items - 3)(return_far)
    seen = catch_up(seen, MESSAGES, event)
    catch_up(had, MESSAGES, handed)

    @pl.when(helped)
    def _():
        for w in range(2):
            landed(far_in.at[w], f_recv.at[w])
            line = far_in[w].astype(f32)
            half = rows // 2
            sums[w, :half] += jnp.exp2(-behinds[w, :half]) * swap_halves(line)
            sums[w, half:] += jnp.exp2(-behinds[w, half:]) * line

    for w in range(2):
        packed[w] = pack(sums[w])
    j = lax.rem(y, CORES)
    returns = []
    for w in range(2):
        column = c if w == 0 else BLOCKS - 1 - c
        returns.append((
            packed.at[w], returned.at[j], o_send.at[w], o_recv.at[j], at(z, column, y // CORES),
            jnp.logical_and(column == y, y // CORES == c),
        ))
    for back in returns:
        deliver(*back)

    @pl.loop(0, MESSAGES)
    def _(e):
        pl.when(up_goes(e))(lambda: up(e).wait_send())
        pl.when(up_comes(e, c))(lambda: pass_up(e).wait_send())
        pl.when(down_goes(e))(lambda: down(e).wait_send())
        pl.when(down_comes(e))(lambda: pass_down(e).wait_send())

    @pl.when(helping)
    def _():
        for copy in far_returns:
            copy.wait_send()

    @pl.when(helped)
    def _():
        for copy in far_queries:
            copy.wait_send()

    net.sent()
    halo_copy.wait_send()
    for parity in range(2):
        pass_own(parity).wait_send()
    for shipment in shipments:
        delivered(*shipment)
    for slot in range(2):
        landed(returned.at[slot], o_recv.at[slot])
    first, second = returned[0].astype(f32), returned[1].astype(f32)
    low = left_lanes(first.shape)
    attn_own[: rows // 2, :] = jnp.where(low, first, swap_halves(second)).astype(bf16)
    attn_own[rows // 2 :, :] = jnp.where(low, swap_halves(first), second).astype(bf16)
    for back in returns:
        delivered(*back)

    attn_net.start()
    conv_net.arrived(4, 7, 8, 9, 10)
    conv_net.sent()
    loads[5].wait()

    @pl.loop(0, rows // step)
    def _(i):
        here = pl.ds(pl.multiple_of(i * step, step), step)
        values = [conv_all[p, here, :] for p in range(pieces)]
        mean = jnp.sum(sum(values[1:], values[0]), axis=1, keepdims=True) / channels
        centered = [v - mean for v in values]
        square = sum([v * v for v in centered[1:]], centered[0] * centered[0])
        spread = jnp.sum(square, axis=1, keepdims=True) / channels
        inverse = lax.rsqrt(spread + epsilon)
        power = jnp.zeros((step, local), f32)
        for p in range(pieces):
            normed = centered[p] * inverse * norm_gain[p : p + 1, :]
            kept = (normed * jax.nn.sigmoid(normed)).astype(bf16).astype(f32)
            power = power + kept * kept
            scaled[here, local * p : local * (p + 1)] = (kept * conv_gain[p : p + 1, :]).astype(bf16)
        scale = lax.rsqrt(jnp.sum(power, axis=1, keepdims=True) / channels + epsilon)
        total[here, :] = jnp.dot(scaled[here, :], out_weights[:channels, :], preferred_element_type=f32) * scale

    def rescale(ref, index, first=False):
        wide = ref[...].astype(f32)
        lanes = pl.ds(pl.multiple_of(index * local, local), local)
        scaled[:, lanes] = (wide * attn_gain[pl.ds(index, 1), :]).astype(bf16)
        if first:
            squares[...] = wide * wide
        else:
            squares[...] += wide * wide

    def rescale_slot(dx, other=False):
        index = attn_net.index(dx, other)
        rescale(attn_all.at[index], index)

    rescale(attn_own, attn_net.index(0), first=True)
    attn_net.relay_first()
    attn_net.arrived(4)
    rescale_slot(0, True)
    attn_net.relay_near()
    rescale_slot(-1)
    rescale_slot(1)
    attn_net.arrived(7)
    rescale_slot(-1, True)
    attn_net.arrived(8)
    rescale_slot(1, True)
    attn_net.relay_far()
    rescale_slot(2)
    attn_net.arrived(9, 10)
    rescale_slot(2, True)

    @pl.loop(0, rows // tile)
    def _(i):
        here = pl.ds(pl.multiple_of(i * tile, tile), tile)
        scale = lax.rsqrt(jnp.sum(squares[here, :], axis=1, keepdims=True) / channels + epsilon)
        product = jnp.dot(scaled[here, :], out_weights[channels:, :], preferred_element_type=f32)
        mixed[here, :] = (total[here, :] + product * scale).astype(bf16)

    attn_net.sent()


def dma(*shape):
    return pltpu.SemaphoreType.DMA(shape)


def per_device(
    tokens, in_gain, conv_a_weight, conv_gate_weight, query_weight, key_weight, value_weight,
    conv_taps, conv_norm_gain, break_shift, conv_out_gain, attn_out_gain, out_weight,
):
    rows, width = tokens.shape
    local = conv_a_weight.shape[1]
    out_width = out_weight.shape[1]
    pieces = RING * CORES
    steps = RowGather.steps
    deep = rows + SHIFT_ROWS
    scratch = [
        VMEM((pieces, rows, width), bf16),
        VMEM((pieces * width, 5 * local), bf16),
        VMEM(out_weight.shape, bf16),
        VMEM((rows, 5 * local), f32),
        VMEM((rows, local), f32),
        VMEM((rows + 32, local), f32),
        VMEM((32, local), f32),
        VMEM((32, local), f32),
        VMEM((2, deep, 128), bf16),
        VMEM((2, rows // 2, 128), bf16),
        VMEM((rows, local), f32),
        VMEM((pieces, rows, local), f32),
        VMEM((PLANES, BLOCKS, deep, 128), bf16),
        VMEM((4, rows // 2, 128), bf16),
        VMEM((4, rows, 128), bf16),
        VMEM((2 + 2 * HELP, rows, 128), f32),
        VMEM((2 + 2 * HELP, rows, 128), f32),
        VMEM((rows, rows), f32),
        VMEM((rows, rows), f32),
        VMEM((rows, rows), bf16),
        VMEM((rows, rows), bf16),
        VMEM((rows, rows), bf16),
        VMEM((rows, rows), bf16),
        VMEM((2, rows // 2, 128), bf16),
        VMEM((2, rows // 2, 128), bf16),
        VMEM((2, rows // 2, 128), bf16),
        VMEM((2, rows // 2, 128), bf16),
        VMEM((rows, local), bf16),
        VMEM((pieces, rows, local), bf16),
        VMEM((rows, pieces * local), bf16),
        VMEM((rows, out_width), f32),
        dma(6), dma(steps), dma(steps), pltpu.SemaphoreType.DMA, pltpu.SemaphoreType.DMA,
        dma(2), dma(2), dma(2), dma(2), dma(4), dma(4),
        dma(MESSAGES), dma(MESSAGES), dma(MESSAGES), dma(MESSAGES),
        dma(MESSAGES), dma(MESSAGES), dma(MESSAGES), dma(MESSAGES),
        dma(2), dma(2), dma(2), dma(2), dma(steps), dma(steps), dma(steps), dma(steps),
    ]
    return pl.pallas_call(
        layer_kernel,
        name="layer",
        out_shape=jax.ShapeDtypeStruct((rows, out_width), bf16),
        in_specs=[pl.BlockSpec(memory_space=VMEM)] * 7 + [pl.BlockSpec(memory_space=pl.ANY)] * 6,
        out_specs=pl.BlockSpec(memory_space=VMEM),
        scratch_shapes=scratch,
        compiler_params=pltpu.CompilerParams(
            collective_id=0, has_side_effects=True, vmem_limit_bytes=60 * 2**20
        ),
    )(
        tokens, in_gain.reshape(2 * pieces, width // 2), break_shift, conv_taps,
        conv_norm_gain.reshape(pieces, local), conv_out_gain.reshape(pieces, local),
        attn_out_gain.reshape(pieces, local),
        conv_a_weight, conv_gate_weight, query_weight, key_weight, value_weight, out_weight,
    )


def solution(mesh):
    columns = P(None, ("fs", "tp"))
    return jax.shard_map(
        per_device,
        mesh=mesh,
        in_specs=(
            P("sp", ("fs", "tp")), P(), columns, columns, columns, columns, columns,
            P(), P(), P(("fs", "tp"), "sp"), P(), P(), columns,
        ),
        out_specs=P("sp", ("fs", "tp")),
        check_vma=False,
    )
```

```python
import jax
import jax.numpy as jnp
from jax import lax
from jax.experimental import pallas as pl
from jax.experimental.pallas import tpu as pltpu
from jax.sharding import PartitionSpec as P

MESH = pl.DeviceIdType.MESH
VMEM = pltpu.VMEM
HEAD = 64
PLANES, BLOCKS, RING, CORES = 8, 4, 4, 2
LOG2E = 1.4426950408889634
MESSAGES, NEAR = 8, 3
HELP = 4
SHIFT_ROWS = 16
epsilon = 1e-06
f32, bf16 = jnp.float32, jnp.bfloat16


def position():
    return lax.axis_index("sp"), lax.axis_index("fs"), lax.axis_index("tp")


def greet(devices):
    barrier = pltpu.get_barrier_semaphore()
    for device in devices:
        pl.semaphore_signal(barrier, inc=1, device_id=device, device_id_type=MESH)
    pl.semaphore_wait(barrier, len(devices))


def remote(src, dst, send, recv, device):
    return pltpu.make_async_remote_copy(
        src_ref=src, dst_ref=dst, send_sem=send, recv_sem=recv, device_id=device, device_id_type=MESH
    )


def left_lanes(shape):
    return lax.broadcasted_iota(jnp.int32, shape, 1) < HEAD


def swap_halves(x):
    return pltpu.roll(x, HEAD, 1)


class RowGather:
    steps = 11

    def __init__(self, own, whole, send, recv):
        self.own, self.whole, self.send, self.recv = own, whole, send, recv
        sp, x, c = position()
        self.x, self.c = x, c
        self.right = (sp, lax.rem(x + 1, RING), c)
        self.left = (sp, lax.rem(x + RING - 1, RING), c)
        self.partner = (sp, x, 1 - c)
        self.half = own.shape[0] // 2

    def index(self, dx, other=False):
        return CORES * lax.rem(self.x + dx + RING, RING) + (1 - self.c if other else self.c)

    def slot(self, dx, other=False, part=None):
        return self.part(self.whole.at[self.index(dx, other)], part)

    def part(self, ref, part):
        return ref if part is None else ref.at[pl.ds(part * self.half, self.half)]

    def out(self, k):
        near = {0: (0, self.right), 1: (1, self.right), 2: (1, self.left), 3: (0, self.left), 4: (None, self.partner)}
        if k in near:
            part, device = near[k]
            src, dst = self.part(self.own, part), self.slot(0, part=part)
        else:
            dx, part, device = {
                5: (-1, 0, self.right),
                6: (1, 1, self.left),
                7: (-1, None, self.partner),
                8: (1, None, self.partner),
                9: (2, 0, self.partner),
                10: (2, 1, self.partner),
            }[k]
            src = dst = self.slot(dx, part=part)
        return remote(src, dst, self.send.at[k], self.recv.at[k], device)

    def arrived(self, *which):
        slots = (
            (-1, False, 0), (-1, False, 1), (1, False, 1), (1, False, 0), (0, True, None), (2, False, 0), (2, False, 1),
            (-1, True, None), (1, True, None), (2, True, 0), (2, True, 1),
        )
        for k in which:
            slot = self.slot(*slots[k])
            remote(slot, slot, self.send.at[k], self.recv.at[k], self.partner).wait_recv()

    def put(self, *which):
        for k in which:
            self.out(k).start()

    def start(self):
        self.put(0, 2, 1, 3, 4)

    def relay_first(self):
        self.arrived(0)
        self.put(5)
        self.arrived(2)
        self.put(6)

    def relay_near(self):
        self.arrived(1)
        self.put(7)
        self.arrived(3)
        self.put(8)

    def relay_far(self):
        self.arrived(5)
        self.put(9)
        self.arrived(6)
        self.put(10)

    def sent(self):
        for k in range(self.steps):
            self.out(k).wait_send()


def landed(ref, sem):
    pltpu.make_async_copy(ref, ref, sem).wait()


def layer_kernel(
    tok, gain, shift, taps, norm_gain, conv_gain, attn_gain, wa, wg, wq, wk, wv, wo,
    mixed,
    tokens_all, stacked, out_weights, acc, squares, padded, tail, halo, kvs, qs, conv_own, conv_all,
    kv_all, q_in, queries, sums, behinds, taken_a, taken_b, fail_a, fail_b, weight_a, weight_b,
    packed, far_packed, far_in, returned, attn_own, attn_all, scaled, total,
    weight_sem, t_send, t_recv, h_send, h_recv, kv_send, kv_recv, pass_send, pass_recv, q_send, q_recv,
    up_send, up_recv, down_send, down_recv, up_pass, up_passed, down_pass, down_passed,
    f_send, f_recv, o_send, o_recv, c_send, c_recv, a_send, a_recv,
):
    sp, x, c = position()
    count = lax.axis_size("sp")
    z, y = sp // BLOCKS, lax.rem(sp, BLOCKS)
    mirror = PLANES - 1 - z
    rows, width = tok.shape
    local = wa.shape[1]
    pieces = RING * CORES
    channels = pieces * local
    model_width = pieces * width

    def at(plane, column, core):
        return (plane * BLOCKS + column, x, core)

    loads = [
        pltpu.make_async_copy(w, stacked.at[:, pl.ds(local * i, local)], weight_sem.at[i])
        for i, w in enumerate((wa, wg, wq, wk, wv))
    ]
    loads.append(pltpu.make_async_copy(wo, out_weights, weight_sem.at[5]))
    for load in loads:
        load.start()

    above, below = lax.rem(z + 1, PLANES), lax.rem(z + PLANES - 1, PLANES)
    partner = at(z, y, 1 - c)
    later_rows = (lax.rem(sp + 1, count), x, c)
    earlier_rows = (lax.rem(sp + count - 1, count), x, c)
    net = RowGather(tok, tokens_all, t_send, t_recv)
    conv_net = RowGather(conv_own, conv_all, c_send, c_recv)
    attn_net = RowGather(attn_own, attn_all, a_send, a_recv)
    peers = [net.right, net.left, at(above, y, c), at(below, y, c), later_rows, earlier_rows]
    for dy in range(BLOCKS):
        for dc in range(CORES):
            if dy or dc:
                peers.append(at(z, lax.rem(y + dy, BLOCKS), lax.rem(c + dc, CORES)))
            peers.append(at(mirror, dy, dc))
    greet(peers)

    net.start()
    shifts = shift[...].astype(f32)
    for head in range(2):
        lines = [shifts[head : head + 1, 128 * k : 128 * (k + 1)] for k in range(rows // 128)]
        lines.append(jnp.zeros((SHIFT_ROWS - len(lines), 128), f32))
        kvs[head, rows : rows + SHIFT_ROWS, :] = jnp.concatenate(lines, axis=0).astype(bf16)
    helped, helping = z >= HELP, z < HELP
    segments = []
    for k in range(NEAR + 2):
        for kind, plane in ((2, z - k), (2, z + k), (0, z - k)):
            if kind and (k > NEAR or (k == 0 and segments)):
                continue
            if kind:
                part = jnp.where(plane < HELP - 1 - z, BLOCKS, jnp.where(plane == HELP - 1 - z, BLOCKS // 2, 0))
                blocks = jnp.where(jnp.logical_and(helping, plane >= 0), 2 * part, 0)
            elif k == 0:
                blocks = jnp.int32(BLOCKS - 1)
            else:
                blocks = jnp.where(plane >= 0, 2 * (BLOCKS if k <= NEAR else BLOCKS // 2), 0)
            segments.append((jnp.int32(k), plane, jnp.int32(kind), blocks))

    def item(i):
        left, (k, plane, kind, place) = i, (jnp.int32(0), z, jnp.int32(0), jnp.int32(0))
        for step_k, step_plane, step_kind, blocks in segments:
            inside = jnp.logical_and(left >= 0, left < blocks)
            k = jnp.where(inside, step_k, k)
            plane = jnp.where(inside, step_plane, plane)
            kind = jnp.where(inside, step_kind, kind)
            place = jnp.where(inside, left, place)
            left = left - blocks
        mine, here = kind == 0, plane == z
        part = jnp.where(plane < HELP - 1 - z, BLOCKS, BLOCKS // 2)
        near_count = jnp.where(here, c, jnp.where(k <= NEAR, BLOCKS, BLOCKS // 2))
        first_count = jnp.where(mine, near_count, part)
        first_top = jnp.where(mine, jnp.where(here, c, BLOCKS), part)
        second_top = jnp.where(mine, jnp.where(here, BLOCKS - 1 - c, BLOCKS), part)
        second = place >= first_count
        block = jnp.where(second, second_top - 1 - (place - first_count), first_top - 1 - place)
        which = kind + jnp.where(second, 1, 0)
        slot = jnp.where(mine, which, 2 + HELP * (which - 2) + plane)
        return k, plane, which, block, slot

    items = (BLOCKS - 1) + BLOCKS * (PLANES - 1)
    so_far, help_end = jnp.int32(0), jnp.int32(-BLOCKS)
    for _, _, kind, blocks in segments:
        so_far = so_far + blocks
        help_end = jnp.where(jnp.logical_and(kind == 2, blocks > 0), so_far, help_end)

    for load in loads[:5]:
        load.wait()
    tile = 128

    def project(ref, index, first=False):
        weights = stacked.at[pl.ds(pl.multiple_of(index * width, width), width)]
        lines = gain[pl.ds(2 * index, 2), :]
        factor = jnp.concatenate([lines[0:1], lines[1:2]], axis=1)

        @pl.loop(0, rows // 256)
        def _(i):
            here = pl.ds(pl.multiple_of(i * 256, 256), 256)
            wide = ref[here, :].astype(f32)
            product = jnp.dot((wide * factor).astype(bf16), weights[...], preferred_element_type=f32)
            square = wide * wide
            square = square[:, : width // 2] + square[:, width // 2 :]
            if first:
                acc[here, :] = product
                squares[here, :] = square
            else:
                acc[here, :] += product
                squares[here, :] += square

    def project_slot(dx, other=False):
        index = net.index(dx, other)
        project(tokens_all.at[index], index)

    project(tok, net.index(0), first=True)
    net.arrived(4)
    project_slot(0, True)
    net.relay_first()
    net.relay_near()
    project_slot(-1)
    project_slot(1)
    net.arrived(7)
    project_slot(-1, True)
    net.arrived(8)
    project_slot(1, True)
    net.relay_far()
    project_slot(2)
    net.arrived(9, 10)
    project_slot(2, True)

    def projected(here, which):
        scale = lax.rsqrt(jnp.sum(squares[here, :], axis=1, keepdims=True) / model_width + epsilon)
        return [(acc[here, pl.ds(local * k, local)] * scale).astype(bf16).astype(f32) for k in which]

    @pl.loop(0, rows // 2 // tile)
    def _(i):
        top = pl.ds(pl.multiple_of(i * tile, tile), tile)
        bottom = pl.ds(pl.multiple_of(rows // 2 + i * tile, tile), tile)
        query_halves = []
        for here in (top, bottom):
            query, key, value = projected(here, (2, 3, 4))
            low = left_lanes(query.shape)
            query_halves.append(query)
            kvs[0, here, :] = jnp.where(low, key, swap_halves(value)).astype(bf16)
            kvs[1, here, :] = jnp.where(low, swap_halves(key), value).astype(bf16)
        first, second = query_halves
        qs[0, top, :] = jnp.where(low, first, swap_halves(second)).astype(bf16)
        qs[1, top, :] = jnp.where(low, swap_halves(first), second).astype(bf16)

    def deliver(src, dst, send, recv, device, mine):
        @pl.when(mine)
        def _():
            pltpu.make_async_copy(src, dst, recv).start()

        @pl.when(jnp.logical_not(mine))
        def _():
            remote(src, dst, send, recv, device).start()

    def delivered(src, dst, send, recv, device, mine):
        @pl.when(jnp.logical_not(mine))
        def _():
            remote(src, dst, send, recv, device).wait_send()

    shipments = []
    for j in range(2):
        head = CORES * c + j
        shipments.append((
            kvs.at[j], kv_all.at[z, y], kv_send.at[j], kv_recv.at[lax.rem(y, CORES)],
            at(z, head, y // CORES), jnp.logical_and(head == y, y // CORES == c),
        ))
    q_core = jnp.where(jnp.logical_or(y == 0, y == BLOCKS - 1), 0, 1)
    q_slot = jnp.where(y < 2, 0, 1)
    far_queries = []
    for j in range(2):
        head = CORES * c + j
        shipments.append((
            qs.at[j], q_in.at[q_slot], q_send.at[j], q_recv.at[q_slot],
            at(z, head, q_core), jnp.logical_and(head == y, q_core == c),
        ))
        far_queries.append(remote(
            qs.at[j], q_in.at[2 + q_slot], q_send.at[2 + j], q_recv.at[2 + q_slot], at(mirror, head, q_core)
        ))
    for shipment in shipments:
        deliver(*shipment)

    @pl.when(helped)
    def _():
        for copy in far_queries:
            copy.start()

    @pl.loop(0, rows // tile)
    def _(i):
        here = pl.ds(pl.multiple_of(i * tile, tile), tile)
        conv_a, conv_gate = projected(here, (0, 1))
        padded[pl.ds(pl.multiple_of(32 + i * tile, 32), tile), :] = conv_a * jax.nn.sigmoid(conv_gate)

    tail[...] = padded[rows : rows + 32, :]
    halo_copy = remote(tail, halo, h_send, h_recv, later_rows)
    halo_copy.start()

    def ring_block(plane, parity):
        return kv_all.at[plane, CORES * c + parity]

    def passed_block(plane, parity):
        return kv_all.at[plane, CORES * (1 - c) + parity]

    def up_plane(k):
        return lax.rem(z - k + PLANES, PLANES)

    def down_plane(k):
        return lax.rem(z + k, PLANES)

    def up(m):
        block = ring_block(up_plane(m // 2), lax.rem(m, 2))
        return remote(block, block, up_send.at[m], up_recv.at[m], at(above, y, c))

    def down(m):
        block = ring_block(down_plane(m // 2), 1 - lax.rem(m, 2))
        return remote(block, block, down_send.at[m], down_recv.at[m], at(below, y, c))

    def pass_up(e):
        block = ring_block(up_plane(e // 2 + 1), lax.rem(e, 2))
        return remote(block, block, up_pass.at[e], up_passed.at[e], partner)

    def pass_down(e):
        block = ring_block(down_plane(e // 2 + 1), 1 - lax.rem(e, 2))
        return remote(block, block, down_pass.at[e], down_passed.at[e], partner)

    def pass_own(parity):
        block = ring_block(z, parity)
        return remote(block, block, pass_send.at[parity], pass_recv.at[parity], partner)

    def rises(plane, k, core):
        return jnp.logical_and(plane >= 0, jnp.logical_or(k < NEAR, core == 1))

    def up_goes(m):
        return jnp.logical_and(rises(z - m // 2, m // 2, c), z < PLANES - 1)

    def up_comes(e, core):
        return rises(z - 1 - e // 2, e // 2, core)

    def down_goes(m):
        return jnp.logical_and(jnp.logical_and(z + m // 2 < HELP, m < 2 * NEAR), z > 0)

    def down_comes(e):
        return jnp.logical_and(z + 1 + e // 2 < HELP, e < 2 * NEAR)

    def send_up(m):
        pl.when(up_goes(m))(lambda: up(m).start())

    def send_down(m):
        pl.when(down_goes(m))(lambda: down(m).start())

    @pl.loop(0, sums.shape[0])
    def _(slot):
        sums[slot] = jnp.zeros((rows, 128), f32)
        behinds[slot] = jnp.zeros((rows, 128), f32)

    for parity in range(2):
        landed(ring_block(z, parity), kv_recv.at[parity])
        send_up(parity)
        pass_own(parity).start()
        if parity == 1:
            send_down(0)
            send_down(1)
    halo_copy.wait_recv()
    padded[0:32, :] = jnp.where(sp == 0, 0.0, halo[...])
    reach = taps.shape[0]
    tap_values = taps[:, pl.ds(pl.multiple_of(net.index(0) * local, local), local)].astype(f32)
    step = 64

    @pl.loop(0, rows // step)
    def _(i):
        window = padded[pl.ds(pl.multiple_of(i * step, step), step + 32), :]
        value = jnp.zeros((step, local), f32)
        for rest in range(8):
            turned = window if rest == 0 else window[rest : rest + step + 24]
            for offset in range(rest, 33, 8):
                tap = offset - (33 - reach)
                if tap >= 0:
                    start = offset - rest
                    value = value + tap_values[tap : tap + 1, :] * turned[start : start + step]
        here = pl.ds(pl.multiple_of(i * step, step), step)
        conv_own[here, :] = value
        conv_all[net.index(0), here, :] = value

    conv_net.start()

    def unpack(slot):
        landed(q_in.at[slot], q_recv.at[slot])
        line = q_in[slot].astype(f32)
        low = left_lanes(line.shape)
        queries[slot, : rows // 2, :] = jnp.where(low, line, 0.0).astype(bf16)
        queries[slot, rows // 2 :, :] = jnp.where(low, swap_halves(line), 0.0).astype(bf16)

    unpack(0)
    unpack(1)
    for parity in range(2):
        landed(passed_block(z, parity), pass_recv.at[parity])

    def event(e):
        @pl.when(up_comes(e, c))
        def _():
            landed(ring_block(up_plane(e // 2 + 1), lax.rem(e, 2)), up_recv.at[e])

            @pl.when(e + 2 < MESSAGES)
            def _():
                send_up(e + 2)

            pass_up(e).start()

        @pl.when(down_comes(e))
        def _():
            landed(ring_block(down_plane(e // 2 + 1), 1 - lax.rem(e, 2)), down_recv.at[e])

            @pl.when(e + 2 < 2 * NEAR)
            def _():
                send_down(e + 2)

            pass_down(e).start()

        for turn, relay in ((1, conv_net.relay_first), (2, conv_net.relay_near), (4, conv_net.relay_far)):
            pl.when(e == turn)(relay)

    def handed(e):
        @pl.when(up_comes(e, 1 - c))
        def _():
            landed(passed_block(up_plane(e // 2 + 1), lax.rem(e, 2)), up_passed.at[e])

        @pl.when(down_comes(e))
        def _():
            landed(passed_block(down_plane(e // 2 + 1), 1 - lax.rem(e, 2)), down_passed.at[e])

    row = lax.broadcasted_iota(jnp.int32, (256, 256), 0)
    column = lax.broadcasted_iota(jnp.int32, (256, 256), 1)
    later = jnp.where(row > column, 1.0, 0.0).astype(bf16)

    def score(which, plane, block, taken, fail, masked=False):
        lines = kv_all[plane, block, rows : rows + SHIFT_ROWS, :].astype(f32) * LOG2E
        line = jnp.concatenate([lines[k : k + 1] for k in range(rows // 128)], axis=1)
        product = lax.dot_general(
            queries[which], kv_all[plane, block, :rows, :], (((1,), (1,)), ((), ())), preferred_element_type=f32
        )
        value = product * (LOG2E * HEAD ** (-0.5)) + line
        lost = jnp.maximum(value, lax.log2(1.0 + jnp.exp2(jnp.minimum(value, 115.0))))
        kept = value - lost
        if masked:
            query_row = lax.broadcasted_iota(jnp.int32, value.shape, 0)
            allowed = lax.broadcasted_iota(jnp.int32, value.shape, 1) < query_row
            lost = jnp.where(allowed, lost, 0.0)
            kept = jnp.where(allowed, kept, -jnp.inf)
        taken[...] = kept
        fail[...] = lost.astype(bf16)

    def weigh(slot, taken, fail, weight):
        half = rows // 2
        near = jnp.dot(fail[:, half:], later, preferred_element_type=f32)
        far = jnp.dot(fail[:, :half], later, preferred_element_type=f32)
        behind = behinds[slot]
        near_total = near[:, 0:1] + fail[:, half : half + 1].astype(f32)
        far_total = far[:, 0:1] + fail[:, 0:1].astype(f32)
        behind_far = behind + jnp.broadcast_to(near_total, behind.shape)
        behinds[slot] = behind_far + jnp.broadcast_to(far_total, behind.shape)
        weight[:, half:] = jnp.exp2(taken[:, half:] - near - jnp.concatenate([behind, behind], axis=1)).astype(bf16)
        weight[:, :half] = jnp.exp2(
            taken[:, :half] - far - jnp.concatenate([behind_far, behind_far], axis=1)
        ).astype(bf16)

    def collect(plane, slot, block, weight):
        sums[slot] += jnp.dot(weight[...], kv_all[plane, block, :rows, :], preferred_element_type=f32)

    far_returns = [
        remote(far_packed.at[w], far_in.at[w], f_send.at[w], f_recv.at[w], at(mirror, y, c)) for w in range(2)
    ]

    def pack(value):
        top, bottom = value[: rows // 2], value[rows // 2 :]
        return jnp.where(left_lanes(top.shape), swap_halves(top), bottom).astype(bf16)

    def return_far():
        for w in range(2):
            base = 2 + HELP * w
            for plane in range(HELP - 2, -1, -1):
                behind = behinds[base + HELP - 1]
                sums[base + HELP - 1] += jnp.exp2(-behind) * sums[base + plane]
                behinds[base + HELP - 1] = behind + behinds[base + plane]
            far_packed[w] = pack(sums[base + HELP - 1])
        for copy in far_returns:
            copy.start()

    def catch_up(done, target, handle):
        lax.fori_loop(done, target, lambda e, _: (handle(e), 0)[1], 0)
        return jnp.maximum(done, target)

    def prepare(i, step_needed, seen, had):
        needed = jnp.minimum(2 * step_needed, MESSAGES)
        expected = jnp.minimum(jnp.maximum(i + 3, 0) // 4, MESSAGES)
        seen = catch_up(seen, jnp.maximum(needed, expected), event)
        had = catch_up(had, needed, handed)
        return seen, had

    @pl.loop(0, 2)
    def _(which):
        block = jnp.where(which == 0, c, BLOCKS - 1 - c)
        score(which, z, block, taken_a, fail_a, masked=True)
        weigh(which, taken_a, fail_a, weight_a)
        collect(z, which, block, weight_a)

    @pl.when(helping)
    def _():
        unpack(2)
        unpack(3)

    zero = jnp.int32(0)
    first, second = item(zero), item(zero + 1)
    seen, had = prepare(zero, second[0], zero, zero)
    score(first[2], first[1], first[3], taken_a, fail_a)
    score(second[2], second[1], second[3], taken_b, fail_b)
    weigh(first[4], taken_a, fail_a, weight_a)

    def stages(now, after, coming, taken, fail, weight, other_taken, other_fail, other_weight):
        weigh(after[4], other_taken, other_fail, other_weight)
        score(coming[2], coming[1], coming[3], taken, fail)
        collect(now[1], now[4], now[3], weight)

    def pair(j, carried):
        now, after, seen, had = carried
        coming, following = item(2 * j + 2), item(2 * j + 3)
        seen, had = prepare(2 * j, jnp.maximum(coming[0], following[0]), seen, had)
        pl.when(jnp.logical_and(help_end > 2 * j - 2, help_end <= 2 * j))(return_far)
        stages(now, after, coming, taken_a, fail_a, weight_a, taken_b, fail_b, weight_b)
        stages(after, coming, following, taken_b, fail_b, weight_b, taken_a, fail_a, weight_a)
        return coming, following, seen, had

    final, _, seen, had = lax.fori_loop(0, (items - 1) // 2, pair, (first, second, seen, had))
    collect(final[1], final[4], final[3], weight_a)
    pl.when(help_end > items - 3)(return_far)
    seen = catch_up(seen, MESSAGES, event)
    catch_up(had, MESSAGES, handed)

    @pl.when(helped)
    def _():
        for w in range(2):
            landed(far_in.at[w], f_recv.at[w])
            line = far_in[w].astype(f32)
            half = rows // 2
            sums[w, :half] += jnp.exp2(-behinds[w, :half]) * swap_halves(line)
            sums[w, half:] += jnp.exp2(-behinds[w, half:]) * line

    for w in range(2):
        packed[w] = pack(sums[w])
    j = lax.rem(y, CORES)
    returns = []
    for w in range(2):
        column = c if w == 0 else BLOCKS - 1 - c
        returns.append((
            packed.at[w], returned.at[j], o_send.at[w], o_recv.at[j], at(z, column, y // CORES),
            jnp.logical_and(column == y, y // CORES == c),
        ))
    for back in returns:
        deliver(*back)

    @pl.loop(0, MESSAGES)
    def _(e):
        pl.when(up_goes(e))(lambda: up(e).wait_send())
        pl.when(up_comes(e, c))(lambda: pass_up(e).wait_send())
        pl.when(down_goes(e))(lambda: down(e).wait_send())
        pl.when(down_comes(e))(lambda: pass_down(e).wait_send())

    @pl.when(helping)
    def _():
        for copy in far_returns:
            copy.wait_send()

    @pl.when(helped)
    def _():
        for copy in far_queries:
            copy.wait_send()

    net.sent()
    halo_copy.wait_send()
    for parity in range(2):
        pass_own(parity).wait_send()
    for shipment in shipments:
        delivered(*shipment)
    conv_net.arrived(4, 7, 8, 9, 10)
    conv_net.sent()
    loads[5].wait()

    @pl.loop(0, rows // step)
    def _(i):
        here = pl.ds(pl.multiple_of(i * step, step), step)
        values = [conv_all[p, here, :] for p in range(pieces)]
        mean = jnp.sum(sum(values[1:], values[0]), axis=1, keepdims=True) / channels
        centered = [v - mean for v in values]
        square = sum([v * v for v in centered[1:]], centered[0] * centered[0])
        spread = jnp.sum(square, axis=1, keepdims=True) / channels
        inverse = lax.rsqrt(spread + epsilon)
        power = jnp.zeros((step, local), f32)
        for p in range(pieces):
            normed = centered[p] * inverse * norm_gain[p : p + 1, :]
            kept = (normed * jax.nn.sigmoid(normed)).astype(bf16).astype(f32)
            power = power + kept * kept
            scaled[here, local * p : local * (p + 1)] = (kept * conv_gain[p : p + 1, :]).astype(bf16)
        scale = lax.rsqrt(jnp.sum(power, axis=1, keepdims=True) / channels + epsilon)
        total[here, :] = jnp.dot(scaled[here, :], out_weights[:channels, :], preferred_element_type=f32) * scale

    for slot in range(2):
        landed(returned.at[slot], o_recv.at[slot])
    first, second = returned[0].astype(f32), returned[1].astype(f32)
    low = left_lanes(first.shape)
    attn_own[: rows // 2, :] = jnp.where(low, first, swap_halves(second)).astype(bf16)
    attn_own[rows // 2 :, :] = jnp.where(low, swap_halves(first), second).astype(bf16)
    for back in returns:
        delivered(*back)

    attn_net.start()
    def rescale(ref, index, first=False):
        wide = ref[...].astype(f32)
        lanes = pl.ds(pl.multiple_of(index * local, local), local)
        scaled[:, lanes] = (wide * attn_gain[pl.ds(index, 1), :]).astype(bf16)
        if first:
            squares[...] = wide * wide
        else:
            squares[...] += wide * wide

    def rescale_slot(dx, other=False):
        index = attn_net.index(dx, other)
        rescale(attn_all.at[index], index)

    rescale(attn_own, attn_net.index(0), first=True)
    attn_net.relay_first()
    attn_net.arrived(4)
    rescale_slot(0, True)
    attn_net.relay_near()
    rescale_slot(-1)
    rescale_slot(1)
    attn_net.arrived(7)
    rescale_slot(-1, True)
    attn_net.arrived(8)
    rescale_slot(1, True)
    attn_net.relay_far()
    rescale_slot(2)
    attn_net.arrived(9, 10)
    rescale_slot(2, True)

    @pl.loop(0, rows // tile)
    def _(i):
        here = pl.ds(pl.multiple_of(i * tile, tile), tile)
        scale = lax.rsqrt(jnp.sum(squares[here, :], axis=1, keepdims=True) / channels + epsilon)
        product = jnp.dot(scaled[here, :], out_weights[channels:, :], preferred_element_type=f32)
        mixed[here, :] = (total[here, :] + product * scale).astype(bf16)

    attn_net.sent()


def dma(*shape):
    return pltpu.SemaphoreType.DMA(shape)


def per_device(
    tokens, in_gain, conv_a_weight, conv_gate_weight, query_weight, key_weight, value_weight,
    conv_taps, conv_norm_gain, break_shift, conv_out_gain, attn_out_gain, out_weight,
):
    rows, width = tokens.shape
    local = conv_a_weight.shape[1]
    out_width = out_weight.shape[1]
    pieces = RING * CORES
    steps = RowGather.steps
    deep = rows + SHIFT_ROWS
    scratch = [
        VMEM((pieces, rows, width), bf16),
        VMEM((pieces * width, 5 * local), bf16),
        VMEM(out_weight.shape, bf16),
        VMEM((rows, 5 * local), f32),
        VMEM((rows, local), f32),
        VMEM((rows + 32, local), f32),
        VMEM((32, local), f32),
        VMEM((32, local), f32),
        VMEM((2, deep, 128), bf16),
        VMEM((2, rows // 2, 128), bf16),
        VMEM((rows, local), f32),
        VMEM((pieces, rows, local), f32),
        VMEM((PLANES, BLOCKS, deep, 128), bf16),
        VMEM((4, rows // 2, 128), bf16),
        VMEM((4, rows, 128), bf16),
        VMEM((2 + 2 * HELP, rows, 128), f32),
        VMEM((2 + 2 * HELP, rows, 128), f32),
        VMEM((rows, rows), f32),
        VMEM((rows, rows), f32),
        VMEM((rows, rows), bf16),
        VMEM((rows, rows), bf16),
        VMEM((rows, rows), bf16),
        VMEM((rows, rows), bf16),
        VMEM((2, rows // 2, 128), bf16),
        VMEM((2, rows // 2, 128), bf16),
        VMEM((2, rows // 2, 128), bf16),
        VMEM((2, rows // 2, 128), bf16),
        VMEM((rows, local), bf16),
        VMEM((pieces, rows, local), bf16),
        VMEM((rows, pieces * local), bf16),
        VMEM((rows, out_width), f32),
        dma(6), dma(steps), dma(steps), pltpu.SemaphoreType.DMA, pltpu.SemaphoreType.DMA,
        dma(2), dma(2), dma(2), dma(2), dma(4), dma(4),
        dma(MESSAGES), dma(MESSAGES), dma(MESSAGES), dma(MESSAGES),
        dma(MESSAGES), dma(MESSAGES), dma(MESSAGES), dma(MESSAGES),
        dma(2), dma(2), dma(2), dma(2), dma(steps), dma(steps), dma(steps), dma(steps),
    ]
    return pl.pallas_call(
        layer_kernel,
        name="layer",
        out_shape=jax.ShapeDtypeStruct((rows, out_width), bf16),
        in_specs=[pl.BlockSpec(memory_space=VMEM)] * 7 + [pl.BlockSpec(memory_space=pl.ANY)] * 6,
        out_specs=pl.BlockSpec(memory_space=VMEM),
        scratch_shapes=scratch,
        compiler_params=pltpu.CompilerParams(
            collective_id=0, has_side_effects=True, vmem_limit_bytes=60 * 2**20
        ),
    )(
        tokens, in_gain.reshape(2 * pieces, width // 2), break_shift, conv_taps,
        conv_norm_gain.reshape(pieces, local), conv_out_gain.reshape(pieces, local),
        attn_out_gain.reshape(pieces, local),
        conv_a_weight, conv_gate_weight, query_weight, key_weight, value_weight, out_weight,
    )


def solution(mesh):
    columns = P(None, ("fs", "tp"))
    return jax.shard_map(
        per_device,
        mesh=mesh,
        in_specs=(
            P("sp", ("fs", "tp")), P(), columns, columns, columns, columns, columns,
            P(), P(), P(("fs", "tp"), "sp"), P(), P(), columns,
        ),
        out_specs=P("sp", ("fs", "tp")),
        check_vma=False,
    )
```

```python
import jax
import jax.numpy as jnp
from jax import lax
from jax.experimental import pallas as pl
from jax.experimental.pallas import tpu as pltpu
from jax.sharding import PartitionSpec as P

MESH = pl.DeviceIdType.MESH
VMEM = pltpu.VMEM
HEAD = 64
PLANES, BLOCKS, RING, CORES = 8, 4, 4, 2
LOG2E = 1.4426950408889634
MESSAGES, NEAR = 8, 3
HELP = 4
SHIFT_ROWS = 16
epsilon = 1e-06
f32, bf16 = jnp.float32, jnp.bfloat16


def position():
    return lax.axis_index("sp"), lax.axis_index("fs"), lax.axis_index("tp")


def greet(devices):
    barrier = pltpu.get_barrier_semaphore()
    for device in devices:
        pl.semaphore_signal(barrier, inc=1, device_id=device, device_id_type=MESH)
    pl.semaphore_wait(barrier, len(devices))


def remote(src, dst, send, recv, device):
    return pltpu.make_async_remote_copy(
        src_ref=src, dst_ref=dst, send_sem=send, recv_sem=recv, device_id=device, device_id_type=MESH
    )


def left_lanes(shape):
    return lax.broadcasted_iota(jnp.int32, shape, 1) < HEAD


def swap_halves(x):
    return pltpu.roll(x, HEAD, 1)


class RowGather:
    steps = 11

    def __init__(self, own, whole, send, recv):
        self.own, self.whole, self.send, self.recv = own, whole, send, recv
        sp, x, c = position()
        self.x, self.c = x, c
        self.right = (sp, lax.rem(x + 1, RING), c)
        self.left = (sp, lax.rem(x + RING - 1, RING), c)
        self.partner = (sp, x, 1 - c)
        self.half = own.shape[0] // 2

    def index(self, dx, other=False):
        return CORES * lax.rem(self.x + dx + RING, RING) + (1 - self.c if other else self.c)

    def slot(self, dx, other=False, part=None):
        return self.part(self.whole.at[self.index(dx, other)], part)

    def part(self, ref, part):
        return ref if part is None else ref.at[pl.ds(part * self.half, self.half)]

    def out(self, k):
        near = {0: (0, self.right), 1: (1, self.right), 2: (1, self.left), 3: (0, self.left), 4: (None, self.partner)}
        if k in near:
            part, device = near[k]
            src, dst = self.part(self.own, part), self.slot(0, part=part)
        else:
            dx, part, device = {
                5: (-1, 0, self.right),
                6: (1, 1, self.left),
                7: (-1, None, self.partner),
                8: (1, None, self.partner),
                9: (2, 0, self.partner),
                10: (2, 1, self.partner),
            }[k]
            src = dst = self.slot(dx, part=part)
        return remote(src, dst, self.send.at[k], self.recv.at[k], device)

    def arrived(self, *which):
        slots = (
            (-1, False, 0), (-1, False, 1), (1, False, 1), (1, False, 0), (0, True, None), (2, False, 0), (2, False, 1),
            (-1, True, None), (1, True, None), (2, True, 0), (2, True, 1),
        )
        for k in which:
            slot = self.slot(*slots[k])
            remote(slot, slot, self.send.at[k], self.recv.at[k], self.partner).wait_recv()

    def put(self, *which):
        for k in which:
            self.out(k).start()

    def start(self):
        self.put(0, 2, 1, 3, 4)

    def relay_first(self):
        self.arrived(0)
        self.put(5)
        self.arrived(2)
        self.put(6)

    def relay_near(self):
        self.arrived(1)
        self.put(7)
        self.arrived(3)
        self.put(8)

    def relay_far(self):
        self.arrived(5)
        self.put(9)
        self.arrived(6)
        self.put(10)

    def sent(self):
        for k in range(self.steps):
            self.out(k).wait_send()


def landed(ref, sem):
    pltpu.make_async_copy(ref, ref, sem).wait()


def layer_kernel(
    tok, gain, shift, taps, norm_gain, conv_gain, attn_gain, wa, wg, wq, wk, wv, wo,
    mixed,
    tokens_all, stacked, out_weights, acc, squares, padded, tail, halo, kvs, qs, conv_own, conv_all,
    kv_all, q_in, queries, sums, behinds, taken_a, taken_b, fail_a, fail_b, weight_a, weight_b,
    packed, far_packed, far_in, returned, attn_own, attn_all, scaled, total, norms,
    weight_sem, t_send, t_recv, h_send, h_recv, kv_send, kv_recv, pass_send, pass_recv, q_send, q_recv,
    up_send, up_recv, down_send, down_recv, up_pass, up_passed, down_pass, down_passed,
    f_send, f_recv, o_send, o_recv, c_send, c_recv, a_send, a_recv,
):
    sp, x, c = position()
    count = lax.axis_size("sp")
    z, y = sp // BLOCKS, lax.rem(sp, BLOCKS)
    mirror = PLANES - 1 - z
    rows, width = tok.shape
    local = wa.shape[1]
    pieces = RING * CORES
    channels = pieces * local
    model_width = pieces * width

    def at(plane, column, core):
        return (plane * BLOCKS + column, x, core)

    loads = [
        pltpu.make_async_copy(w, stacked.at[:, pl.ds(local * i, local)], weight_sem.at[i])
        for i, w in enumerate((wa, wg, wq, wk, wv))
    ]
    loads.append(pltpu.make_async_copy(wo, out_weights, weight_sem.at[5]))
    for load in loads:
        load.start()

    above, below = lax.rem(z + 1, PLANES), lax.rem(z + PLANES - 1, PLANES)
    partner = at(z, y, 1 - c)
    later_rows = (lax.rem(sp + 1, count), x, c)
    earlier_rows = (lax.rem(sp + count - 1, count), x, c)
    net = RowGather(tok, tokens_all, t_send, t_recv)
    conv_net = RowGather(conv_own, conv_all, c_send, c_recv)
    attn_net = RowGather(attn_own, attn_all, a_send, a_recv)
    peers = [net.right, net.left, at(above, y, c), at(below, y, c), later_rows, earlier_rows]
    for dy in range(BLOCKS):
        for dc in range(CORES):
            if dy or dc:
                peers.append(at(z, lax.rem(y + dy, BLOCKS), lax.rem(c + dc, CORES)))
            peers.append(at(mirror, dy, dc))
    greet(peers)

    net.start()
    shifts = shift[...].astype(f32)
    for head in range(2):
        lines = [shifts[head : head + 1, 128 * k : 128 * (k + 1)] for k in range(rows // 128)]
        lines.append(jnp.zeros((SHIFT_ROWS - len(lines), 128), f32))
        kvs[head, rows : rows + SHIFT_ROWS, :] = jnp.concatenate(lines, axis=0).astype(bf16)
    helped, helping = z >= HELP, z < HELP
    segments = []
    for k in range(NEAR + 2):
        for kind, plane in ((2, z - k), (2, z + k), (0, z - k)):
            if kind and (k > NEAR or (k == 0 and segments)):
                continue
            if kind:
                part = jnp.where(plane < HELP - 1 - z, BLOCKS, jnp.where(plane == HELP - 1 - z, BLOCKS // 2, 0))
                blocks = jnp.where(jnp.logical_and(helping, plane >= 0), 2 * part, 0)
            elif k == 0:
                blocks = jnp.int32(BLOCKS - 1)
            else:
                blocks = jnp.where(plane >= 0, 2 * (BLOCKS if k <= NEAR else BLOCKS // 2), 0)
            segments.append((jnp.int32(k), plane, jnp.int32(kind), blocks))

    def item(i):
        left, (k, plane, kind, place) = i, (jnp.int32(0), z, jnp.int32(0), jnp.int32(0))
        for step_k, step_plane, step_kind, blocks in segments:
            inside = jnp.logical_and(left >= 0, left < blocks)
            k = jnp.where(inside, step_k, k)
            plane = jnp.where(inside, step_plane, plane)
            kind = jnp.where(inside, step_kind, kind)
            place = jnp.where(inside, left, place)
            left = left - blocks
        mine, here = kind == 0, plane == z
        part = jnp.where(plane < HELP - 1 - z, BLOCKS, BLOCKS // 2)
        near_count = jnp.where(here, c, jnp.where(k <= NEAR, BLOCKS, BLOCKS // 2))
        first_count = jnp.where(mine, near_count, part)
        first_top = jnp.where(mine, jnp.where(here, c, BLOCKS), part)
        second_top = jnp.where(mine, jnp.where(here, BLOCKS - 1 - c, BLOCKS), part)
        second = place >= first_count
        block = jnp.where(second, second_top - 1 - (place - first_count), first_top - 1 - place)
        which = kind + jnp.where(second, 1, 0)
        slot = jnp.where(mine, which, 2 + HELP * (which - 2) + plane)
        return k, plane, which, block, slot

    items = (BLOCKS - 1) + BLOCKS * (PLANES - 1)
    so_far, help_end = jnp.int32(0), jnp.int32(-BLOCKS)
    for _, _, kind, blocks in segments:
        so_far = so_far + blocks
        help_end = jnp.where(jnp.logical_and(kind == 2, blocks > 0), so_far, help_end)

    for load in loads[:5]:
        load.wait()
    tile = 128

    def project(ref, index, first=False):
        weights = stacked.at[pl.ds(pl.multiple_of(index * width, width), width)]
        lines = gain[pl.ds(2 * index, 2), :]
        factor = jnp.concatenate([lines[0:1], lines[1:2]], axis=1)

        @pl.loop(0, rows // 256)
        def _(i):
            here = pl.ds(pl.multiple_of(i * 256, 256), 256)
            wide = ref[here, :].astype(f32)
            product = jnp.dot((wide * factor).astype(bf16), weights[...], preferred_element_type=f32)
            square = wide * wide
            square = square[:, : width // 2] + square[:, width // 2 :]
            if first:
                acc[here, :] = product
                squares[here, :] = square
            else:
                acc[here, :] += product
                squares[here, :] += square

    def project_slot(dx, other=False):
        index = net.index(dx, other)
        project(tokens_all.at[index], index)

    project(tok, net.index(0), first=True)
    net.arrived(4)
    project_slot(0, True)
    net.relay_first()
    net.relay_near()
    project_slot(-1)
    project_slot(1)
    net.arrived(7)
    project_slot(-1, True)
    net.relay_far()
    net.arrived(8)
    project_slot(1, True)
    project_slot(2)
    net.arrived(9, 10)
    project_slot(2, True)

    def projected(here, which):
        scale = lax.rsqrt(jnp.sum(squares[here, :], axis=1, keepdims=True) / model_width + epsilon)
        return [(acc[here, pl.ds(local * k, local)] * scale).astype(bf16).astype(f32) for k in which]

    @pl.loop(0, rows // 2 // tile)
    def _(i):
        top = pl.ds(pl.multiple_of(i * tile, tile), tile)
        bottom = pl.ds(pl.multiple_of(rows // 2 + i * tile, tile), tile)
        query_halves = []
        for here in (top, bottom):
            query, key, value = projected(here, (2, 3, 4))
            low = left_lanes(query.shape)
            query_halves.append(query)
            kvs[0, here, :] = jnp.where(low, key, swap_halves(value)).astype(bf16)
            kvs[1, here, :] = jnp.where(low, swap_halves(key), value).astype(bf16)
        first, second = query_halves
        qs[0, top, :] = jnp.where(low, first, swap_halves(second)).astype(bf16)
        qs[1, top, :] = jnp.where(low, swap_halves(first), second).astype(bf16)

    def deliver(src, dst, send, recv, device, mine):
        @pl.when(mine)
        def _():
            pltpu.make_async_copy(src, dst, recv).start()

        @pl.when(jnp.logical_not(mine))
        def _():
            remote(src, dst, send, recv, device).start()

    def delivered(src, dst, send, recv, device, mine):
        @pl.when(jnp.logical_not(mine))
        def _():
            remote(src, dst, send, recv, device).wait_send()

    shipments = []
    for j in range(2):
        head = CORES * c + j
        shipments.append((
            kvs.at[j], kv_all.at[z, y], kv_send.at[j], kv_recv.at[lax.rem(y, CORES)],
            at(z, head, y // CORES), jnp.logical_and(head == y, y // CORES == c),
        ))
    q_core = jnp.where(jnp.logical_or(y == 0, y == BLOCKS - 1), 0, 1)
    q_slot = jnp.where(y < 2, 0, 1)
    far_queries = []
    for j in range(2):
        head = CORES * c + j
        shipments.append((
            qs.at[j], q_in.at[q_slot], q_send.at[j], q_recv.at[q_slot],
            at(z, head, q_core), jnp.logical_and(head == y, q_core == c),
        ))
        far_queries.append(remote(
            qs.at[j], q_in.at[2 + q_slot], q_send.at[2 + j], q_recv.at[2 + q_slot], at(mirror, head, q_core)
        ))
    for shipment in shipments:
        deliver(*shipment)

    @pl.when(helped)
    def _():
        for copy in far_queries:
            copy.start()

    @pl.loop(0, rows // tile)
    def _(i):
        here = pl.ds(pl.multiple_of(i * tile, tile), tile)
        conv_a, conv_gate = projected(here, (0, 1))
        padded[pl.ds(pl.multiple_of(32 + i * tile, 32), tile), :] = conv_a * jax.nn.sigmoid(conv_gate)

    tail[...] = padded[rows : rows + 32, :]
    halo_copy = remote(tail, halo, h_send, h_recv, later_rows)
    halo_copy.start()

    def ring_block(plane, parity):
        return kv_all.at[plane, CORES * c + parity]

    def passed_block(plane, parity):
        return kv_all.at[plane, CORES * (1 - c) + parity]

    def up_plane(k):
        return lax.rem(z - k + PLANES, PLANES)

    def down_plane(k):
        return lax.rem(z + k, PLANES)

    def up(m):
        block = ring_block(up_plane(m // 2), lax.rem(m, 2))
        return remote(block, block, up_send.at[m], up_recv.at[m], at(above, y, c))

    def down(m):
        block = ring_block(down_plane(m // 2), 1 - lax.rem(m, 2))
        return remote(block, block, down_send.at[m], down_recv.at[m], at(below, y, c))

    def pass_up(e):
        block = ring_block(up_plane(e // 2 + 1), lax.rem(e, 2))
        return remote(block, block, up_pass.at[e], up_passed.at[e], partner)

    def pass_down(e):
        block = ring_block(down_plane(e // 2 + 1), 1 - lax.rem(e, 2))
        return remote(block, block, down_pass.at[e], down_passed.at[e], partner)

    def pass_own(parity):
        block = ring_block(z, parity)
        return remote(block, block, pass_send.at[parity], pass_recv.at[parity], partner)

    def rises(plane, k, core):
        return jnp.logical_and(plane >= 0, jnp.logical_or(k < NEAR, core == 1))

    def up_goes(m):
        return jnp.logical_and(rises(z - m // 2, m // 2, c), z < PLANES - 1)

    def up_comes(e, core):
        return rises(z - 1 - e // 2, e // 2, core)

    def down_goes(m):
        return jnp.logical_and(jnp.logical_and(z + m // 2 < HELP, m < 2 * NEAR), z > 0)

    def down_comes(e):
        return jnp.logical_and(z + 1 + e // 2 < HELP, e < 2 * NEAR)

    def send_up(m):
        pl.when(up_goes(m))(lambda: up(m).start())

    def send_down(m):
        pl.when(down_goes(m))(lambda: down(m).start())

    @pl.loop(0, sums.shape[0])
    def _(slot):
        sums[slot] = jnp.zeros((rows, 128), f32)
        behinds[slot] = jnp.zeros((rows, 128), f32)

    for parity in range(2):
        landed(ring_block(z, parity), kv_recv.at[parity])
        send_up(parity)
        pass_own(parity).start()
        if parity == 1:
            send_down(0)
            send_down(1)
    halo_copy.wait_recv()
    padded[0:32, :] = jnp.where(sp == 0, 0.0, halo[...])
    reach = taps.shape[0]
    tap_values = taps[:, pl.ds(pl.multiple_of(net.index(0) * local, local), local)].astype(f32)
    step = 64

    @pl.loop(0, rows // step)
    def _(i):
        window = padded[pl.ds(pl.multiple_of(i * step, step), step + 32), :]
        value = jnp.zeros((step, local), f32)
        for rest in range(8):
            turned = window if rest == 0 else window[rest : rest + step + 24]
            for offset in range(rest, 33, 8):
                tap = offset - (33 - reach)
                if tap >= 0:
                    start = offset - rest
                    value = value + tap_values[tap : tap + 1, :] * turned[start : start + step]
        here = pl.ds(pl.multiple_of(i * step, step), step)
        conv_own[here, :] = value
        conv_all[net.index(0), here, :] = value

    conv_net.start()

    def unpack(slot):
        landed(q_in.at[slot], q_recv.at[slot])
        line = q_in[slot].astype(f32)
        low = left_lanes(line.shape)
        queries[slot, : rows // 2, :] = jnp.where(low, line, 0.0).astype(bf16)
        queries[slot, rows // 2 :, :] = jnp.where(low, swap_halves(line), 0.0).astype(bf16)

    unpack(0)
    unpack(1)
    for parity in range(2):
        landed(passed_block(z, parity), pass_recv.at[parity])

    def event(e):
        @pl.when(up_comes(e, c))
        def _():
            landed(ring_block(up_plane(e // 2 + 1), lax.rem(e, 2)), up_recv.at[e])

            @pl.when(e + 2 < MESSAGES)
            def _():
                send_up(e + 2)

            pass_up(e).start()

        @pl.when(down_comes(e))
        def _():
            landed(ring_block(down_plane(e // 2 + 1), 1 - lax.rem(e, 2)), down_recv.at[e])

            @pl.when(e + 2 < 2 * NEAR)
            def _():
                send_down(e + 2)

            pass_down(e).start()

        for turn, relay in ((1, conv_net.relay_first), (2, conv_net.relay_near), (4, conv_net.relay_far)):
            pl.when(e == turn)(relay)

    def handed(e):
        @pl.when(up_comes(e, 1 - c))
        def _():
            landed(passed_block(up_plane(e // 2 + 1), lax.rem(e, 2)), up_passed.at[e])

        @pl.when(down_comes(e))
        def _():
            landed(passed_block(down_plane(e // 2 + 1), 1 - lax.rem(e, 2)), down_passed.at[e])

    row = lax.broadcasted_iota(jnp.int32, (256, 256), 0)
    column = lax.broadcasted_iota(jnp.int32, (256, 256), 1)
    later = jnp.where(row > column, 1.0, 0.0).astype(bf16)

    def score(which, plane, block, taken, fail, masked=False):
        lines = kv_all[plane, block, rows : rows + SHIFT_ROWS, :].astype(f32) * LOG2E
        line = jnp.concatenate([lines[k : k + 1] for k in range(rows // 128)], axis=1)
        product = lax.dot_general(
            queries[which], kv_all[plane, block, :rows, :], (((1,), (1,)), ((), ())), preferred_element_type=f32
        )
        value = product * (LOG2E * HEAD ** (-0.5)) + line
        lost = jnp.maximum(value, lax.log2(1.0 + jnp.exp2(jnp.minimum(value, 115.0))))
        kept = value - lost
        if masked:
            query_row = lax.broadcasted_iota(jnp.int32, value.shape, 0)
            allowed = lax.broadcasted_iota(jnp.int32, value.shape, 1) < query_row
            lost = jnp.where(allowed, lost, 0.0)
            kept = jnp.where(allowed, kept, -jnp.inf)
        taken[...] = kept
        fail[...] = lost.astype(bf16)

    def weigh(slot, taken, fail, weight):
        half = rows // 2
        near = jnp.dot(fail[:, half:], later, preferred_element_type=f32)
        far = jnp.dot(fail[:, :half], later, preferred_element_type=f32)
        behind = behinds[slot]
        near_total = near[:, 0:1] + fail[:, half : half + 1].astype(f32)
        far_total = far[:, 0:1] + fail[:, 0:1].astype(f32)
        behind_far = behind + jnp.broadcast_to(near_total, behind.shape)
        behinds[slot] = behind_far + jnp.broadcast_to(far_total, behind.shape)
        weight[:, half:] = jnp.exp2(taken[:, half:] - near - jnp.concatenate([behind, behind], axis=1)).astype(bf16)
        weight[:, :half] = jnp.exp2(
            taken[:, :half] - far - jnp.concatenate([behind_far, behind_far], axis=1)
        ).astype(bf16)

    def collect(plane, slot, block, weight):
        sums[slot] += jnp.dot(weight[...], kv_all[plane, block, :rows, :], preferred_element_type=f32)

    far_returns = [
        remote(far_packed.at[w], far_in.at[w], f_send.at[w], f_recv.at[w], at(mirror, y, c)) for w in range(2)
    ]

    def pack(value):
        top, bottom = value[: rows // 2], value[rows // 2 :]
        return jnp.where(left_lanes(top.shape), swap_halves(top), bottom).astype(bf16)

    def return_far():
        for w in range(2):
            base = 2 + HELP * w
            for plane in range(HELP - 2, -1, -1):
                behind = behinds[base + HELP - 1]
                sums[base + HELP - 1] += jnp.exp2(-behind) * sums[base + plane]
                behinds[base + HELP - 1] = behind + behinds[base + plane]
            far_packed[w] = pack(sums[base + HELP - 1])
        for copy in far_returns:
            copy.start()

    def catch_up(done, target, handle):
        lax.fori_loop(done, target, lambda e, _: (handle(e), 0)[1], 0)
        return jnp.maximum(done, target)

    def prepare(i, step_needed, seen, had):
        needed = jnp.minimum(2 * step_needed, MESSAGES)
        expected = jnp.minimum(jnp.maximum(i + 3, 0) // 4, MESSAGES)
        seen = catch_up(seen, jnp.maximum(needed, expected), event)
        had = catch_up(had, needed, handed)
        return seen, had

    @pl.loop(0, 2)
    def _(which):
        block = jnp.where(which == 0, c, BLOCKS - 1 - c)
        score(which, z, block, taken_a, fail_a, masked=True)
        weigh(which, taken_a, fail_a, weight_a)
        collect(z, which, block, weight_a)

    @pl.when(helping)
    def _():
        unpack(2)
        unpack(3)

    zero = jnp.int32(0)
    first, second = item(zero), item(zero + 1)
    seen, had = prepare(zero, second[0], zero, zero)
    score(first[2], first[1], first[3], taken_a, fail_a)
    score(second[2], second[1], second[3], taken_b, fail_b)
    weigh(first[4], taken_a, fail_a, weight_a)

    def stages(now, after, coming, taken, fail, weight, other_taken, other_fail, other_weight):
        weigh(after[4], other_taken, other_fail, other_weight)
        score(coming[2], coming[1], coming[3], taken, fail)
        collect(now[1], now[4], now[3], weight)

    def pair(j, carried):
        now, after, seen, had = carried
        coming, following = item(2 * j + 2), item(2 * j + 3)
        seen, had = prepare(2 * j, jnp.maximum(coming[0], following[0]), seen, had)
        pl.when(jnp.logical_and(help_end > 2 * j - 2, help_end <= 2 * j))(return_far)
        stages(now, after, coming, taken_a, fail_a, weight_a, taken_b, fail_b, weight_b)
        stages(after, coming, following, taken_b, fail_b, weight_b, taken_a, fail_a, weight_a)
        return coming, following, seen, had

    final, _, seen, had = lax.fori_loop(0, (items - 1) // 2, pair, (first, second, seen, had))
    collect(final[1], final[4], final[3], weight_a)
    pl.when(help_end > items - 3)(return_far)
    seen = catch_up(seen, MESSAGES, event)
    catch_up(had, MESSAGES, handed)

    @pl.when(helped)
    def _():
        for w in range(2):
            landed(far_in.at[w], f_recv.at[w])
            line = far_in[w].astype(f32)
            half = rows // 2
            sums[w, :half] += jnp.exp2(-behinds[w, :half]) * swap_halves(line)
            sums[w, half:] += jnp.exp2(-behinds[w, half:]) * line

    for w in range(2):
        packed[w] = pack(sums[w])
    j = lax.rem(y, CORES)
    returns = []
    for w in range(2):
        column = c if w == 0 else BLOCKS - 1 - c
        returns.append((
            packed.at[w], returned.at[j], o_send.at[w], o_recv.at[j], at(z, column, y // CORES),
            jnp.logical_and(column == y, y // CORES == c),
        ))
    for back in returns:
        deliver(*back)

    @pl.loop(0, MESSAGES)
    def _(e):
        pl.when(up_goes(e))(lambda: up(e).wait_send())
        pl.when(up_comes(e, c))(lambda: pass_up(e).wait_send())
        pl.when(down_goes(e))(lambda: down(e).wait_send())
        pl.when(down_comes(e))(lambda: pass_down(e).wait_send())

    @pl.when(helping)
    def _():
        for copy in far_returns:
            copy.wait_send()

    @pl.when(helped)
    def _():
        for copy in far_queries:
            copy.wait_send()

    net.sent()
    halo_copy.wait_send()
    for parity in range(2):
        pass_own(parity).wait_send()
    for shipment in shipments:
        delivered(*shipment)
    conv_net.arrived(4, 7, 8, 9, 10)
    conv_net.sent()
    loads[5].wait()

    @pl.loop(0, rows // step)
    def _(i):
        here = pl.ds(pl.multiple_of(i * step, step), step)
        values = [conv_all[p, here, :] for p in range(pieces)]
        mean = jnp.sum(sum(values[1:], values[0]), axis=1, keepdims=True) / channels
        centered = [v - mean for v in values]
        square = sum([v * v for v in centered[1:]], centered[0] * centered[0])
        spread = jnp.sum(square, axis=1, keepdims=True) / channels
        inverse = lax.rsqrt(spread + epsilon)
        power = jnp.zeros((step, local), f32)
        for p in range(pieces):
            normed = centered[p] * inverse * norm_gain[p : p + 1, :]
            kept = (normed * jax.nn.sigmoid(normed)).astype(bf16).astype(f32)
            power = power + kept * kept
            scaled[here, local * p : local * (p + 1)] = (kept * conv_gain[p : p + 1, :]).astype(bf16)
        scale = lax.rsqrt(jnp.sum(power, axis=1, keepdims=True) / channels + epsilon)
        norms[here, :] = jnp.broadcast_to(scale, (step, 128))

    for slot in range(2):
        landed(returned.at[slot], o_recv.at[slot])
    first, second = returned[0].astype(f32), returned[1].astype(f32)
    low = left_lanes(first.shape)
    attn_own[: rows // 2, :] = jnp.where(low, first, swap_halves(second)).astype(bf16)
    attn_own[rows // 2 :, :] = jnp.where(low, swap_halves(first), second).astype(bf16)
    for back in returns:
        delivered(*back)

    attn_net.start()
    @pl.loop(0, rows // 256)
    def _(i):
        here = pl.ds(pl.multiple_of(i * 256, 256), 256)
        product = jnp.dot(scaled[here, :], out_weights[:channels, :], preferred_element_type=f32)
        total[here, :] = product * jnp.concatenate([norms[here, :], norms[here, :]], axis=1)

    def rescale(ref, index, first=False):
        wide = ref[...].astype(f32)
        lanes = pl.ds(pl.multiple_of(index * local, local), local)
        scaled[:, lanes] = (wide * attn_gain[pl.ds(index, 1), :]).astype(bf16)
        if first:
            squares[...] = wide * wide
        else:
            squares[...] += wide * wide

    def rescale_slot(dx, other=False):
        index = attn_net.index(dx, other)
        rescale(attn_all.at[index], index)

    rescale(attn_own, attn_net.index(0), first=True)
    attn_net.relay_first()
    attn_net.arrived(4)
    rescale_slot(0, True)
    attn_net.relay_near()
    rescale_slot(-1)
    rescale_slot(1)
    attn_net.arrived(7)
    rescale_slot(-1, True)
    attn_net.arrived(8)
    rescale_slot(1, True)
    attn_net.relay_far()
    rescale_slot(2)
    attn_net.arrived(9, 10)
    rescale_slot(2, True)

    @pl.loop(0, rows // 256)
    def _(i):
        here = pl.ds(pl.multiple_of(i * 256, 256), 256)
        scale = lax.rsqrt(jnp.sum(squares[here, :], axis=1, keepdims=True) / channels + epsilon)
        product = jnp.dot(scaled[here, :], out_weights[channels:, :], preferred_element_type=f32)
        mixed[here, :] = (total[here, :] + product * scale).astype(bf16)

    attn_net.sent()


def dma(*shape):
    return pltpu.SemaphoreType.DMA(shape)


def per_device(
    tokens, in_gain, conv_a_weight, conv_gate_weight, query_weight, key_weight, value_weight,
    conv_taps, conv_norm_gain, break_shift, conv_out_gain, attn_out_gain, out_weight,
):
    rows, width = tokens.shape
    local = conv_a_weight.shape[1]
    out_width = out_weight.shape[1]
    pieces = RING * CORES
    steps = RowGather.steps
    deep = rows + SHIFT_ROWS
    scratch = [
        VMEM((pieces, rows, width), bf16),
        VMEM((pieces * width, 5 * local), bf16),
        VMEM(out_weight.shape, bf16),
        VMEM((rows, 5 * local), f32),
        VMEM((rows, local), f32),
        VMEM((rows + 32, local), f32),
        VMEM((32, local), f32),
        VMEM((32, local), f32),
        VMEM((2, deep, 128), bf16),
        VMEM((2, rows // 2, 128), bf16),
        VMEM((rows, local), f32),
        VMEM((pieces, rows, local), f32),
        VMEM((PLANES, BLOCKS, deep, 128), bf16),
        VMEM((4, rows // 2, 128), bf16),
        VMEM((4, rows, 128), bf16),
        VMEM((2 + 2 * HELP, rows, 128), f32),
        VMEM((2 + 2 * HELP, rows, 128), f32),
        VMEM((rows, rows), f32),
        VMEM((rows, rows), f32),
        VMEM((rows, rows), bf16),
        VMEM((rows, rows), bf16),
        VMEM((rows, rows), bf16),
        VMEM((rows, rows), bf16),
        VMEM((2, rows // 2, 128), bf16),
        VMEM((2, rows // 2, 128), bf16),
        VMEM((2, rows // 2, 128), bf16),
        VMEM((2, rows // 2, 128), bf16),
        VMEM((rows, local), bf16),
        VMEM((pieces, rows, local), bf16),
        VMEM((rows, pieces * local), bf16),
        VMEM((rows, out_width), f32),
        VMEM((rows, 128), f32),
        dma(6), dma(steps), dma(steps), pltpu.SemaphoreType.DMA, pltpu.SemaphoreType.DMA,
        dma(2), dma(2), dma(2), dma(2), dma(4), dma(4),
        dma(MESSAGES), dma(MESSAGES), dma(MESSAGES), dma(MESSAGES),
        dma(MESSAGES), dma(MESSAGES), dma(MESSAGES), dma(MESSAGES),
        dma(2), dma(2), dma(2), dma(2), dma(steps), dma(steps), dma(steps), dma(steps),
    ]
    return pl.pallas_call(
        layer_kernel,
        name="layer",
        out_shape=jax.ShapeDtypeStruct((rows, out_width), bf16),
        in_specs=[pl.BlockSpec(memory_space=VMEM)] * 7 + [pl.BlockSpec(memory_space=pl.ANY)] * 6,
        out_specs=pl.BlockSpec(memory_space=VMEM),
        scratch_shapes=scratch,
        compiler_params=pltpu.CompilerParams(
            collective_id=0, has_side_effects=True, vmem_limit_bytes=60 * 2**20
        ),
    )(
        tokens, in_gain.reshape(2 * pieces, width // 2), break_shift, conv_taps,
        conv_norm_gain.reshape(pieces, local), conv_out_gain.reshape(pieces, local),
        attn_out_gain.reshape(pieces, local),
        conv_a_weight, conv_gate_weight, query_weight, key_weight, value_weight, out_weight,
    )


def solution(mesh):
    columns = P(None, ("fs", "tp"))
    return jax.shard_map(
        per_device,
        mesh=mesh,
        in_specs=(
            P("sp", ("fs", "tp")), P(), columns, columns, columns, columns, columns,
            P(), P(), P(("fs", "tp"), "sp"), P(), P(), columns,
        ),
        out_specs=P("sp", ("fs", "tp")),
        check_vma=False,
    )
```
